128 devices in a mesh: ep: 64 (over z, y, x), tp: 2 (over core).
Axes of the slice: x: 4, y: 4, z: 4, core: 2. Of those that a mesh axis runs over, the one named last changes fastest.
Arguments:
- tokens: bfloat16 [16384, 2048], P('ep'), may hold values from -16 to 16
- expert_ids: int32 [16384, 4], P('ep'), may hold values from 0 to 63, all different within a row; in each aligned block of 256 rows (0 to 255, 256 to 511, ...) at most 24 rows name the same one
- gates: float32 [16384, 4], P('ep'), may hold values from 0.05 to 0.6
- cotangent: bfloat16 [16384, 2048], P('ep'), may hold values from -16 to 16
- w_gate: bfloat16 [64, 2048, 512], P('ep', None, 'tp'), may hold values from -0.125 to 0.125
- w_up: bfloat16 [64, 2048, 512], P('ep', None, 'tp'), may hold values from -0.125 to 0.125
- w_down: bfloat16 [64, 512, 2048], P('ep', 'tp'), may hold values from -0.25 to 0.25
- sh_gate: bfloat16 [2048, 512], P(None, 'tp'), may hold values from -0.125 to 0.125
- sh_up: bfloat16 [2048, 512], P(None, 'tp'), may hold values from -0.125 to 0.125
- sh_down: bfloat16 [512, 2048], P('tp'), may hold values from -0.25 to 0.25
Outputs:
- token_grad: bfloat16 [16384, 2048], P('ep', 'tp')
- gate_grad: float32 [16384, 4], P('ep')
- expert_gate_grad: float32 [64, 2048, 512], P('ep', None, 'tp')
- expert_up_grad: float32 [64, 2048, 512], P('ep', None, 'tp')
- expert_down_grad: float32 [64, 512, 2048], P('ep', 'tp')
- shared_gate_grad: float32 [2048, 512], P('ep', 'tp')
- shared_up_grad: float32 [2048, 512], P('ep', 'tp')
- shared_down_grad: float32 [512, 2048], P('tp', 'ep')
- expert_gate_rows: float32 [64, 2048], P('ep')
- expert_up_rows: float32 [64, 2048], P('ep')
- expert_down_rows: float32 [64, 512], P('ep', 'tp')
- shared_gate_rows: float32 [2048], P('ep')
- shared_up_rows: float32 [2048], P('ep')
- shared_down_rows: float32 [512], P('tp')
The draws below stay inside these ranges and needn't reach their ends.
Inputs may be any that keep to these rules, and one draw needn't show every extreme that they name: `expert_ids`: each row names 4 different experts. Within each aligned block of 256 tokens no expert is named by more than 24 assignments, a bound that is reached in some blocks.
All inputs are finite; a program needn't handle non-finite values.
Results may differ from the reference program's by a relative error of at most 0.0085.
Values may be sent and summed in bfloat16 or wider, within the bound.
No kernel may reach another device: no remote copies, remote signals or barrier semaphores. Data moves between devices by JAX's collectives and lax.ppermute only.
A program may use at most 128 MiB of HBM per device.

```python
import math
import jax
import jax.numpy as jnp
import numpy as np
from jax import lax

D = 2048
HID = 512
SH = 512
TOP_K = 4
TOK_DEV = 256
EXPERTS = 64
CAP = 24
TOKENS = 16384
N_TP = 2


def with_spikes(values, stream_key, source, target, parts, factor):
    def block_of(position):
        return (jnp.arange(values.shape[position]) // (values.shape[position] // parts)).reshape((-1,) + (1,) * (values.ndim - 1 - position))

    first = jax.random.permutation(stream_key, parts)[block_of(target)]
    second = (block_of(target) + parts // 2) % parts
    return jnp.where((block_of(source) == first) | (block_of(source) == second), factor * values, values)


def levels(stream_key, shape, split, least, high):
    def one(dim, shards_of):
        steps = jax.random.uniform(jax.random.fold_in(jax.random.fold_in(stream_key, 6), dim), (shards_of,), jnp.float32, least / len(split), high / len(split))
        return jnp.repeat(jnp.exp(steps), shape[dim] // shards_of).reshape((-1,) + (1,) * (len(shape) - dim - 1))

    loudness = one(*split[0])
    for cut in split[1:]:
        loudness = loudness * one(*cut)
    return loudness


def deal_out(stream_key, own, number, rows, amount, top, reach, skew):
    ranking = jax.random.permutation(stream_key, amount)
    crowded, ordinary = load_shares(amount, rows * top, reach, skew, True), load_shares(amount, rows * top, reach, skew, False)
    places = jnp.arange(amount)

    def named(sizes, offset_by):
        used = int((sizes > 0).sum())
        fixed = max(1, used // 4)
        passed = fixed + (places - fixed + offset_by * (used - fixed)) % max(1, amount - fixed)
        return jnp.zeros((amount,), jnp.int32).at[ranking[jnp.where(places < fixed, places, passed)]].set(jnp.asarray(sizes, jnp.int32))

    sizes = jnp.where(number % 4 == 0, named(crowded, number // 4), named(ordinary, number - number // 4 - 1))
    mixed = jax.random.permutation(jax.random.fold_in(own, 3), amount)
    giver, sink = mixed[0:amount // 2 * 2:2], mixed[1:amount // 2 * 2:2]
    room = jnp.minimum(sizes[giver] - 1, reach - sizes[sink]) // 2
    room = jnp.where((giver == ranking[0]) | (sink == ranking[0]) | (sizes[sink] == 0), 0, jnp.maximum(room, 0))
    passed = jax.random.randint(jax.random.fold_in(own, 4), (amount // 2,), 0, 1 << 20) % (room + 1)
    sizes = sizes.at[giver].add(-passed).at[sink].add(passed)
    members = jnp.searchsorted(jnp.cumsum(sizes), jnp.arange(rows * top), side="right").astype(jnp.int32)
    grid = members.reshape(top, rows).T
    grid = grid[jax.random.permutation(jax.random.fold_in(own, 1), rows)]
    offset_by = jax.random.randint(jax.random.fold_in(own, 2), (rows, 1), 0, top)
    return jnp.take_along_axis(grid, (jnp.arange(top)[None, :] + offset_by) % top, axis=1)


def load_shares(count, total, most, skew, full):
    weights = [(1 << 20) // math.isqrt(grade ** skew) + 1 for grade in range(1, count + 1)]
    largest = most if full else min(most, max(-(-total // count), total * weights[0] // sum(weights)))
    least = 1 if total - largest >= count - 1 else 0
    given, spare = [largest] + [least] * (count - 1), total - largest - least * (count - 1)
    while spare > 0:
        movable = [i for i in range(1, count) if given[i] < largest] or [i for i in range(1, count) if given[i] < most]
        mass, remaining = sum([weights[i] for i in movable]), spare
        for i in movable:
            addition = min(most - given[i], max(1, remaining * weights[i] // mass), spare)
            given[i] = given[i] + addition
            spare = spare - addition
    return np.array(given)


def bell_draw(key, shape, deviation, reach, shards=(), kind=jnp.bfloat16):
    array = deviation * jax.random.normal(key, shape, jnp.float32)
    if shards:
        array = array * levels(key, shape, shards, -0.22, 0.18)
    return jnp.clip(array, -reach, reach).astype(kind)


def noise_with(key, extent, deviation, bound, cuts, heavy, kind=jnp.bfloat16):
    values = deviation * jax.random.normal(key, extent, jnp.float32)
    if cuts:
        values = values * levels(key, extent, cuts, -0.22, 0.18)
    return jnp.clip(with_spikes(values, jax.random.fold_in(key, 3), *heavy), -bound, bound).astype(kind)


def setup_inputs(seed: int = 0) -> dict:
    keys = jax.random.split(jax.random.key(seed), 11)
    tokens = noise_with(keys[0], (TOKENS, D), 1.0, 16.0, ((0, 64),), (0, 1, 64, 4.0))
    expert_ids_keys = jax.random.split(jax.random.fold_in(keys[1], 1), TOKENS // TOK_DEV)
    expert_ids_turns = jax.random.permutation(jax.random.fold_in(keys[1], 3), TOKENS // TOK_DEV)
    expert_ids = jax.vmap(lambda own, number: deal_out(jax.random.fold_in(keys[1], 2), own, number, TOK_DEV, EXPERTS, TOP_K, CAP, 2))(expert_ids_keys, expert_ids_turns).reshape((TOKENS, TOP_K))
    gates = jnp.clip(0.05 + 0.55 * jax.random.uniform(keys[2], (TOKENS, TOP_K), jnp.float32) ** levels(keys[2], (TOKENS, TOP_K), ((0, 64),), -0.2, 0.2), 0.05, 0.6)
    cotangent = noise_with(keys[3], (TOKENS, D), 1.0, 16.0, ((0, 64),), (0, 1, 64, 4.0))
    w_gate = bell_draw(keys[4], (EXPERTS, D, HID), D ** -0.5, 0.125, ((0, 64), (2, 2)))
    w_up = bell_draw(keys[5], (EXPERTS, D, HID), D ** -0.5, 0.125, ((0, 64), (2, 2)))
    w_down = bell_draw(keys[6], (EXPERTS, HID, D), HID ** -0.5, 0.25, ((0, 64), (1, 2)))
    sh_gate = bell_draw(keys[7], (D, SH), D ** -0.5, 0.125, ((1, 2),))
    sh_up = bell_draw(keys[8], (D, SH), D ** -0.5, 0.125, ((1, 2),))
    sh_down = bell_draw(keys[9], (SH, D), SH ** -0.5, 0.25, ((0, 2),))
    return dict(tokens=tokens, expert_ids=expert_ids, gates=gates, cotangent=cotangent, w_gate=w_gate, w_up=w_up, w_down=w_down, sh_gate=sh_gate, sh_up=sh_up, sh_down=sh_down)


def silu_parts(pre):
    sigmoid = jax.nn.sigmoid(pre)
    return pre * sigmoid, sigmoid * (1.0 + pre * (1.0 - sigmoid))


def halves_sum(left_a, right_a, left_b, right_b, pieces):
    step_cols = left_a.shape[1] // pieces
    total = jnp.zeros((left_a.shape[0], right_a.shape[0]), jnp.float32)
    for piece in range(pieces):
        first_col = piece * step_cols
        part = jnp.dot(left_a[:, first_col:first_col + step_cols], right_a[:, first_col:first_col + step_cols].T, preferred_element_type=jnp.float32)
        part = part + jnp.dot(left_b[:, first_col:first_col + step_cols], right_b[:, first_col:first_col + step_cols].T, preferred_element_type=jnp.float32)
        total = total + lax.optimization_barrier(part.astype(jnp.bfloat16)).astype(jnp.float32)
    return total


def backward_rows(inputs, cot_rows, w_g, w_u, w_d):
    gate_pre = jnp.dot(inputs, w_g, preferred_element_type=jnp.float32)
    up_pre = jnp.dot(inputs, w_u, preferred_element_type=jnp.float32)
    active, slope = silu_parts(gate_pre)
    hidden = (active * up_pre).astype(jnp.bfloat16)
    hidden_cot = jnp.dot(cot_rows, w_d.T, preferred_element_type=jnp.float32)
    gate_sum = jnp.sum(hidden.astype(jnp.float32) * hidden_cot, axis=1)
    d_gate = (hidden_cot * up_pre * slope).astype(jnp.bfloat16)
    d_up = (hidden_cot * active).astype(jnp.bfloat16)
    grad_g = jnp.dot(inputs.T, d_gate, preferred_element_type=jnp.float32)
    grad_u = jnp.dot(inputs.T, d_up, preferred_element_type=jnp.float32)
    grad_d = jnp.dot(hidden.T, cot_rows, preferred_element_type=jnp.float32)
    rows = halves_sum(d_gate, w_g, d_up, w_u, N_TP)
    return grad_g, grad_u, grad_d, rows, gate_sum


def reference(tokens, expert_ids, gates, cotangent, w_gate, w_up, w_down, sh_gate, sh_up, sh_down):
    per_dev = TOK_DEV * TOP_K
    assign = TOKENS * TOP_K
    slots = EXPERTS * CAP
    flat_ids = expert_ids.reshape(EXPERTS, per_dev).astype(jnp.int32)
    onehot = (flat_ids[:, :, None] == jnp.arange(EXPERTS, dtype=jnp.int32)[None, None, :]).astype(jnp.int32)
    slot_rank = jnp.sum((jnp.cumsum(onehot, axis=1) - 1) * onehot, axis=2)
    sources = jnp.arange(EXPERTS, dtype=jnp.int32)[:, None]
    slot_row = (flat_ids * slots + sources * CAP + slot_rank).reshape(assign).astype(jnp.int32)
    slot_table = jnp.full((EXPERTS * slots,), assign, jnp.int32).at[slot_row].set(jnp.arange(assign, dtype=jnp.int32))
    filled = slot_table < assign
    source = jnp.minimum(slot_table, assign - 1)
    token_row = (source // TOP_K).astype(jnp.int32)
    slot_gate = jnp.where(filled, gates.reshape(assign)[source], jnp.zeros((), jnp.float32))

    def one_expert(packed):
        rows_index, gate_col, keep, w_g, w_u, w_d = packed
        inputs = jnp.where(keep[:, None], tokens[rows_index], jnp.zeros((), tokens.dtype))
        cot_rows = (gate_col[:, None] * cotangent[rows_index].astype(jnp.float32)).astype(jnp.bfloat16)
        return backward_rows(inputs, cot_rows, w_g, w_u, w_d)

    grad_g, grad_u, grad_d, slot_rows, gate_sums = lax.map(one_expert, (token_row.reshape(EXPERTS, slots), slot_gate.reshape(EXPERTS, slots), filled.reshape(EXPERTS, slots), w_gate, w_up, w_down))
    flat_rows = slot_rows.reshape(EXPERTS * slots, D)
    picks = slot_row.reshape(TOKENS, TOP_K)
    routed = jnp.zeros((TOKENS, D), jnp.float32)
    for column in range(TOP_K):
        routed = routed + flat_rows[picks[:, column]].astype(jnp.float32)
    gate_grad = gate_sums.reshape(EXPERTS * slots)[picks] / gates
    shared_g, shared_u, shared_d, shared_rows, unused = backward_rows(tokens, cotangent, sh_gate, sh_up, sh_down)
    token_grad = (routed + shared_rows).astype(jnp.bfloat16)
    return (token_grad, gate_grad, grad_g, grad_u, grad_d, shared_g, shared_u, shared_d,
            jnp.sum(grad_g * grad_g, axis=2), jnp.sum(grad_u * grad_u, axis=2), jnp.sum(grad_d * grad_d, axis=2),
            jnp.sum(shared_g * shared_g, axis=1), jnp.sum(shared_u * shared_u, axis=1), jnp.sum(shared_d * shared_d, axis=1))
```

```python
import jax
import jax.numpy as jnp
from jax import lax
from jax.sharding import PartitionSpec as P

F32 = jnp.float32
BF16 = jnp.bfloat16
ROWS = (((0,), (0,)), ((), ()))
COLS = (((1,), (1,)), ((), ()))
PLAIN = (((1,), (0,)), ((), ()))


def mm(a, b, contract=PLAIN):
    return lax.dot_general(a, b, contract, preferred_element_type=F32)


def swap(x):
    return lax.ppermute(x, "tp", [(0, 1), (1, 0)])


def to_each(x):
    return lax.all_to_all(x, "ep", 0, 0, tiled=True)


def silu_parts(pre):
    sigmoid = jax.nn.sigmoid(pre)
    return (pre * sigmoid, sigmoid * (1.0 + pre * (1.0 - sigmoid)))


def to_hidden(inputs, cots, w_g, w_u, w_d):
    gate_pre = mm(inputs, w_g)
    up_pre = mm(inputs, w_u)
    active, slope = silu_parts(gate_pre)
    hidden = (active * up_pre).astype(BF16)
    hidden_cot = mm(cots, w_d, COLS)
    gate_part = jnp.sum(hidden.astype(F32) * hidden_cot, axis=1)
    d_gate = (hidden_cot * up_pre * slope).astype(BF16)
    d_up = (hidden_cot * active).astype(BF16)
    return hidden, d_gate, d_up, gate_part


def input_rows(d_gate, d_up, w_g, w_u, first, width):
    part_g = lax.dynamic_slice_in_dim(w_g, first, width, 0)
    part_u = lax.dynamic_slice_in_dim(w_u, first, width, 0)
    return (mm(d_gate, part_g, COLS) + mm(d_up, part_u, COLS)).astype(BF16)


def local(tokens, expert_ids, gates, cotangent, w_gate, w_up, w_down, sh_gate, sh_up, sh_down):
    experts = lax.axis_size("ep")
    tok_rows, width = tokens.shape
    top = expert_ids.shape[1]
    cap = 3 * tok_rows * top // (2 * experts)
    slots = experts * cap
    half = width // 2
    tp = lax.axis_index("tp")
    own, other = tp * half, (1 - tp) * half
    w_g, w_u, w_d = w_gate[0], w_up[0], w_down[0]

    ids_t = expert_ids.T
    names = [ids_t[k][None, :] == jnp.arange(experts, dtype=jnp.int32)[:, None] for k in range(top)]
    hit = names[0]
    for name in names[1:]:
        hit = hit | name
    order = jnp.arange(tok_rows)
    before = (order[:, None] < order[None, :]).astype(BF16)
    rank = mm(hit.astype(BF16), before)
    place = jnp.where(hit, rank, -1.0)
    pick = place[:, None, :] == jnp.arange(cap, dtype=F32)[None, :, None]
    select = pick.astype(BF16).reshape(slots, tok_rows)
    gates_t = gates.T
    gate_of = sum(jnp.where(names[k], gates_t[k][None, :], 0.0) for k in range(top))
    slot_gate = jnp.sum(jnp.where(pick, gate_of[:, None, :], 0.0), axis=2).reshape(slots)

    both = jnp.concatenate(
        [
            lax.dynamic_slice_in_dim(tokens, own, half, 1),
            lax.dynamic_slice_in_dim(cotangent, own, half, 1),
        ],
        axis=1,
    )
    is_cot = jnp.arange(width) >= half
    scale = jnp.where(is_cot[None, :], slot_gate[:, None], 1.0)
    sent = (mm(select, both) * scale).astype(BF16)
    got = to_each(sent.reshape(experts, cap, width)).reshape(slots, width)
    peer = swap(got)
    low = tp == 0
    inputs = jnp.concatenate(
        [jnp.where(low, got[:, :half], peer[:, :half]), jnp.where(low, peer[:, :half], got[:, :half])],
        axis=1,
    )
    cots = jnp.concatenate(
        [jnp.where(low, got[:, half:], peer[:, half:]), jnp.where(low, peer[:, half:], got[:, half:])],
        axis=1,
    )

    s_hidden, s_gate, s_up, unused = to_hidden(tokens, cotangent, sh_gate, sh_up, sh_down)
    shared = jnp.concatenate(
        [mm(tokens, s_gate, ROWS), mm(tokens, s_up, ROWS), mm(cotangent, s_hidden, ROWS)], axis=1
    ).astype(BF16)
    hid = s_hidden.shape[1]
    shared_got = to_each(shared.reshape(experts, width // experts, 3 * hid))
    shared_sum = jnp.sum(shared_got.astype(F32), axis=0)
    shared_g, shared_u = shared_sum[:, :hid], shared_sum[:, hid : 2 * hid]
    shared_d = shared_sum[:, 2 * hid :].T
    s_rows = swap(input_rows(s_gate, s_up, sh_gate, sh_up, other, half)).astype(F32) + input_rows(
        s_gate, s_up, sh_gate, sh_up, own, half
    ).astype(F32)

    hidden, d_gate, d_up, gate_part = to_hidden(inputs, cots, w_g, w_u, w_d)
    from_peer = swap(input_rows(d_gate, d_up, w_g, w_u, other, half))
    kept = input_rows(d_gate, d_up, w_g, w_u, own, half)
    slot_rows = (from_peer.astype(F32) + kept.astype(F32)).astype(BF16)
    back_rows = to_each(slot_rows.reshape(experts, cap, half)).reshape(slots, half)

    grad_g = mm(inputs, d_gate, ROWS)
    grad_u = mm(inputs, d_up, ROWS)
    grad_d = mm(hidden, cots, ROWS)

    gate_sum = gate_part + swap(gate_part)
    down_part = jnp.sum(shared_d * shared_d, axis=1)
    small = jnp.concatenate(
        [gate_sum.reshape(experts, cap), jnp.broadcast_to(down_part[None], (experts, hid))], axis=1
    )
    small = to_each(small)
    back_gate = small[:, :cap]
    down_norms = jnp.sum(small[:, cap:], axis=0)

    norms = jnp.concatenate(
        [
            jnp.sum(grad_g * grad_g, axis=1),
            jnp.sum(grad_u * grad_u, axis=1),
            jnp.sum(shared_g * shared_g, axis=1),
            jnp.sum(shared_u * shared_u, axis=1),
        ]
    )
    norms = norms + swap(norms)
    step = width // experts
    gate_norms, up_norms = norms[:width], norms[width : 2 * width]
    shared_gate_norms, shared_up_norms = norms[2 * width : 2 * width + step], norms[2 * width + step :]

    routed = mm(select, back_rows, ROWS)
    token_grad = (routed + s_rows).astype(BF16)
    gate_at = jnp.sum(jnp.where(pick, back_gate[:, :, None], 0.0), axis=1)
    gate_grad = (
        jnp.stack([jnp.sum(jnp.where(name, gate_at, 0.0), axis=0) for name in names], axis=1) / gates
    )
    return (
        token_grad,
        gate_grad,
        grad_g[None],
        grad_u[None],
        grad_d[None],
        shared_g,
        shared_u,
        shared_d,
        gate_norms[None],
        up_norms[None],
        jnp.sum(grad_d * grad_d, axis=1)[None],
        shared_gate_norms,
        shared_up_norms,
        down_norms,
    )


def solution(mesh):
    placed = (
        P("ep", None),
        P("ep", None),
        P("ep", None),
        P("ep", None),
        P("ep", None, "tp"),
        P("ep", None, "tp"),
        P("ep", "tp", None),
        P(None, "tp"),
        P(None, "tp"),
        P("tp", None),
    )
    return jax.shard_map(
        local,
        mesh=mesh,
        in_specs=placed,
        out_specs=(
            P("ep", "tp"),
            P("ep", None),
            P("ep", None, "tp"),
            P("ep", None, "tp"),
            P("ep", "tp", None),
            P("ep", "tp"),
            P("ep", "tp"),
            P("tp", "ep"),
            P("ep", None),
            P("ep", None),
            P("ep", "tp"),
            P("ep"),
            P("ep"),
            P("tp"),
        ),
        check_vma=False,
    )
```

```python
import jax
import jax.numpy as jnp
from jax import lax
from jax.sharding import PartitionSpec as P


F32 = jnp.float32
BF16 = jnp.bfloat16
ROWS = (((0,), (0,)), ((), ()))
COLS = (((1,), (1,)), ((), ()))
PLAIN = (((1,), (0,)), ((), ()))


def mm(a, b, contract=PLAIN):
    return lax.dot_general(a, b, contract, preferred_element_type=F32)


def swap(x):
    return lax.ppermute(x, "tp", [(0, 1), (1, 0)])


def to_each(x):
    return lax.all_to_all(x, "ep", 0, 0, tiled=True)


def silu_parts(pre):
    sigmoid = jax.nn.sigmoid(pre)
    return (pre * sigmoid, sigmoid * (1.0 + pre * (1.0 - sigmoid)))


def to_hidden(inputs, cots, w_g, w_u, w_d):
    gate_pre = mm(inputs, w_g)
    up_pre = mm(inputs, w_u)
    active, slope = silu_parts(gate_pre)
    hidden = (active * up_pre).astype(BF16)
    hidden_cot = mm(cots, w_d, COLS)
    gate_part = jnp.sum(hidden.astype(F32) * hidden_cot, axis=1)
    d_gate = (hidden_cot * up_pre * slope).astype(BF16)
    d_up = (hidden_cot * active).astype(BF16)
    return hidden, d_gate, d_up, gate_part


def input_rows(d_both, w_both, first, width):
    return mm(d_both, lax.dynamic_slice_in_dim(w_both, first, width, 0), COLS).astype(BF16)


def layer(tokens, expert_ids, gates, cotangent, w_gate, w_up, w_down, sh_gate, sh_up, sh_down):
    experts = lax.axis_size("ep")
    tok_rows, width = tokens.shape
    top = expert_ids.shape[1]
    cap = 3 * tok_rows * top // (2 * experts)
    slots = experts * cap
    half = width // 2
    tp = lax.axis_index("tp")
    own, other = tp * half, (1 - tp) * half
    w_g, w_u, w_d = w_gate[0], w_up[0], w_down[0]

    ids_t = expert_ids.T
    names = [ids_t[k][None, :] == jnp.arange(experts, dtype=jnp.int32)[:, None] for k in range(top)]
    hit = names[0]
    for name in names[1:]:
        hit = hit | name
    order = jnp.arange(tok_rows)
    before = (order[:, None] < order[None, :]).astype(BF16)
    rank = mm(hit.astype(BF16), before)
    place = jnp.where(hit, rank, -1.0)
    pick = place[:, None, :] == jnp.arange(cap, dtype=F32)[None, :, None]
    select = pick.astype(BF16).reshape(slots, tok_rows)
    gates_t = gates.T
    gate_of = sum(jnp.where(names[k], gates_t[k][None, :], 0.0) for k in range(top))
    slot_gate = jnp.sum(jnp.where(pick, gate_of[:, None, :], 0.0), axis=2).reshape(slots)

    both = jnp.concatenate(
        [
            lax.dynamic_slice_in_dim(tokens, own, half, 1),
            lax.dynamic_slice_in_dim(cotangent, own, half, 1),
        ],
        axis=1,
    )
    is_cot = jnp.arange(width) >= half
    scale = jnp.where(is_cot[None, :], slot_gate[:, None], 1.0)
    sent = (mm(select, both) * scale).astype(BF16)
    got = to_each(sent.reshape(experts, cap, width)).reshape(slots, width)

    s_hidden, s_gate, s_up, _ = to_hidden(tokens, cotangent, sh_gate, sh_up, sh_down)
    hid = s_hidden.shape[1]
    s_both = jnp.concatenate([sh_gate, sh_up], axis=1)
    s_d = jnp.concatenate([s_gate, s_up], axis=1)
    s_other = input_rows(s_d, s_both, other, half)
    s_own = input_rows(s_d, s_both, own, half)
    shared = jnp.concatenate([mm(tokens, s_d, ROWS), mm(cotangent, s_hidden, ROWS)], axis=1).astype(BF16)
    shared_got = to_each(shared.reshape(experts, width // experts, 3 * hid))
    s_peer = swap(s_other)
    w_gu = jnp.concatenate([w_g, w_u], axis=1)
    w_gu_own = lax.dynamic_slice_in_dim(w_gu, own, half, 0)
    w_gu_other = lax.dynamic_slice_in_dim(w_gu, other, half, 0)
    w_d_own = lax.dynamic_slice_in_dim(w_d, own, half, 1)
    w_d_other = lax.dynamic_slice_in_dim(w_d, other, half, 1)

    peer = swap(got)
    pre = mm(got[:, :half], w_gu_own) + mm(peer[:, :half], w_gu_other)
    hidden_cot = mm(got[:, half:], w_d_own, COLS) + mm(peer[:, half:], w_d_other, COLS)
    gate_pre, up_pre = pre[:, :hid], pre[:, hid:]
    active, slope = silu_parts(gate_pre)
    hidden = (active * up_pre).astype(BF16)
    gate_part = jnp.sum(hidden.astype(F32) * hidden_cot, axis=1)
    d_both = jnp.concatenate([hidden_cot * up_pre * slope, hidden_cot * active], axis=1).astype(BF16)
    rows_other = mm(d_both, w_gu_other, COLS).astype(BF16)
    rows_own = mm(d_both, w_gu_own, COLS).astype(BF16)
    from_peer = swap(rows_other)
    gate_peer = swap(gate_part)
    slot_rows = (from_peer.astype(F32) + rows_own.astype(F32)).astype(BF16)
    back_rows = to_each(slot_rows.reshape(experts, cap, half)).reshape(slots, half)

    low = tp == 0
    inputs = jnp.concatenate(
        [jnp.where(low, got[:, :half], peer[:, :half]), jnp.where(low, peer[:, :half], got[:, :half])],
        axis=1,
    )
    cots = jnp.concatenate(
        [jnp.where(low, got[:, half:], peer[:, half:]), jnp.where(low, peer[:, half:], got[:, half:])],
        axis=1,
    )
    grad_g = mm(inputs, d_both[:, :hid], ROWS)
    grad_u = mm(inputs, d_both[:, hid:], ROWS)
    grad_d = mm(hidden, cots, ROWS)

    shared_sum = jnp.sum(shared_got.astype(F32), axis=0)
    shared_g, shared_u = shared_sum[:, :hid], shared_sum[:, hid : 2 * hid]
    shared_d = shared_sum[:, 2 * hid :].T
    down_part = jnp.sum(shared_d * shared_d, axis=1)
    s_rows = s_peer.astype(F32) + s_own.astype(F32)
    gate_sum = gate_part + gate_peer
    small = jnp.concatenate(
        [gate_sum.reshape(experts, cap), jnp.broadcast_to(down_part[None], (experts, hid))], axis=1
    )
    small = to_each(small)
    back_gate = small[:, :cap]
    down_norms = jnp.sum(small[:, cap:], axis=0)

    norms = jnp.concatenate(
        [
            jnp.sum(grad_g * grad_g, axis=1),
            jnp.sum(grad_u * grad_u, axis=1),
            jnp.sum(shared_g * shared_g, axis=1),
            jnp.sum(shared_u * shared_u, axis=1),
        ]
    )
    norms = norms + swap(norms)
    step = width // experts
    gate_norms, up_norms = norms[:width], norms[width : 2 * width]
    shared_gate_norms, shared_up_norms = norms[2 * width : 2 * width + step], norms[2 * width + step :]

    routed = mm(select, back_rows, ROWS)
    token_grad = (routed + s_rows).astype(BF16)
    gate_at = jnp.sum(jnp.where(pick, back_gate[:, :, None], 0.0), axis=1)
    gate_grad = (
        jnp.stack([jnp.sum(jnp.where(name, gate_at, 0.0), axis=0) for name in names], axis=1) / gates
    )
    return (
        token_grad,
        gate_grad,
        grad_g[None],
        grad_u[None],
        grad_d[None],
        shared_g,
        shared_u,
        shared_d,
        gate_norms[None],
        up_norms[None],
        jnp.sum(grad_d * grad_d, axis=1)[None],
        shared_gate_norms,
        shared_up_norms,
        down_norms,
    )


def solution(mesh):
    placed = (
        P("ep", None),
        P("ep", None),
        P("ep", None),
        P("ep", None),
        P("ep", None, "tp"),
        P("ep", None, "tp"),
        P("ep", "tp", None),
        P(None, "tp"),
        P(None, "tp"),
        P("tp", None),
    )
    return jax.shard_map(
        layer,
        mesh=mesh,
        in_specs=placed,
        out_specs=(
            P("ep", "tp"),
            P("ep", None),
            P("ep", None, "tp"),
            P("ep", None, "tp"),
            P("ep", "tp", None),
            P("ep", "tp"),
            P("ep", "tp"),
            P("tp", "ep"),
            P("ep", None),
            P("ep", None),
            P("ep", "tp"),
            P("ep"),
            P("ep"),
            P("tp"),
        ),
        check_vma=False,
    )
```

```python
import jax
import jax.numpy as jnp
from jax import lax
from jax.sharding import PartitionSpec as P


F32 = jnp.float32
BF16 = jnp.bfloat16
ROWS = (((0,), (0,)), ((), ()))
COLS = (((1,), (1,)), ((), ()))
PLAIN = (((1,), (0,)), ((), ()))


def mm(a, b, contract=PLAIN):
    return lax.dot_general(a, b, contract, preferred_element_type=F32)


def swap(x):
    return lax.ppermute(x, "tp", [(0, 1), (1, 0)])


def coords(axis):
    size = lax.axis_size("ep")
    side = round(size ** (1 / 3))
    stride = (side * side, side, 1)[axis]
    return size, side, stride


def shifted(x, axis, by):
    size, side, stride = coords(axis)
    pairs = []
    for i in range(size):
        c = i // stride % side
        pairs.append((i, i + ((c + by) % side - c) * stride))
    return lax.ppermute(x, "ep", pairs)


def wrap(i, size):
    return lax.rem(i, size)


def own_coord(axis):
    _, side, stride = coords(axis)
    return wrap(lax.div(lax.axis_index("ep"), stride), side)


def summed_over(x, axes):
    left = [0, 1, 2]
    for axis in axes:
        dim = left.index(axis)
        left.remove(axis)
        _, side, _ = coords(axis)
        c = own_coord(axis)
        total = lax.dynamic_index_in_dim(x, c, dim, keepdims=False).astype(F32)
        for by in range(1, side):
            piece = lax.dynamic_index_in_dim(x, wrap(c + by, side), dim, keepdims=False)
            total = total + shifted(piece, axis, by).astype(F32)
        x = total if not left else total.astype(BF16)
    return x


def far_and_wide(rows, part):
    size, side, _ = coords(0)
    i = jnp.arange(size, dtype=jnp.int32)
    parts = [wrap(lax.div(i, coords(axis)[2]), side) for axis in range(3)]
    there = sum(wrap(own_coord(a) + parts[a], side) * coords(a)[2] for a in range(3))
    back = sum(wrap(own_coord(a) + side - parts[a], side) * coords(a)[2] for a in range(3))
    cols = rows.shape[1]
    table = exact_rows(there, rows).reshape(side, side, side, cols)
    for axis in range(3):
        out, parts = [], []
        for by in range(1, side):
            piece = lax.index_in_dim(table, by, axis, keepdims=False)
            sent = jnp.concatenate([piece.reshape(-1), part])
            came = shifted(sent, axis, by)
            out.append(came[: piece.size].reshape(piece.shape))
            parts.append(came[piece.size :])
        kept = lax.index_in_dim(table, 0, axis, keepdims=False)
        table = jnp.stack([kept] + out, axis=axis)
        part = (part + parts[1]) + (parts[0] + parts[2])
    onto = (back[None, :] == i[:, None]).astype(F32)
    rows = lax.dot_general(onto, table.reshape(size, cols), PLAIN, precision=lax.Precision.HIGHEST)
    return rows, part


def exact_rows(index, rows):
    onehot = (index[:, None] == jnp.arange(rows.shape[0])[None, :]).astype(F32)
    return lax.dot_general(onehot, rows, PLAIN, precision=lax.Precision.HIGHEST)


def to_each(x):
    return lax.all_to_all(x, "ep", 0, 0, tiled=True)


def silu_parts(pre):
    sigmoid = jax.nn.sigmoid(pre)
    return (pre * sigmoid, sigmoid * (1.0 + pre * (1.0 - sigmoid)))


def to_hidden(inputs, cots, w_g, w_u, w_d):
    gate_pre = mm(inputs, w_g)
    up_pre = mm(inputs, w_u)
    active, slope = silu_parts(gate_pre)
    hidden = (active * up_pre).astype(BF16)
    hidden_cot = mm(cots, w_d, COLS)
    gate_part = jnp.sum(hidden.astype(F32) * hidden_cot, axis=1)
    d_gate = (hidden_cot * up_pre * slope).astype(BF16)
    d_up = (hidden_cot * active).astype(BF16)
    return hidden, d_gate, d_up, gate_part


def input_rows(d_both, w_both, first, width):
    return mm(d_both, lax.dynamic_slice_in_dim(w_both, first, width, 0), COLS).astype(BF16)


def layer(tokens, expert_ids, gates, cotangent, w_gate, w_up, w_down, sh_gate, sh_up, sh_down):
    experts = lax.axis_size("ep")
    tok_rows, width = tokens.shape
    top = expert_ids.shape[1]
    cap = 3 * tok_rows * top // (2 * experts)
    slots = experts * cap
    half = width // 2
    tp = lax.axis_index("tp")
    own, other = tp * half, (1 - tp) * half
    w_g, w_u, w_d = w_gate[0], w_up[0], w_down[0]

    ids_t = expert_ids.T
    names = [ids_t[k][None, :] == jnp.arange(experts, dtype=jnp.int32)[:, None] for k in range(top)]
    hit = names[0]
    for name in names[1:]:
        hit = hit | name
    order = jnp.arange(tok_rows)
    before = (order[:, None] < order[None, :]).astype(BF16)
    rank = mm(hit.astype(BF16), before)
    place = jnp.where(hit, rank, -1.0)
    pick = place[:, None, :] == jnp.arange(cap, dtype=F32)[None, :, None]
    select = pick.astype(BF16).reshape(slots, tok_rows)
    gates_t = gates.T
    gate_of = sum(jnp.where(names[k], gates_t[k][None, :], 0.0) for k in range(top))
    slot_gate = jnp.sum(jnp.where(pick, gate_of[:, None, :], 0.0), axis=2).reshape(slots)

    both = jnp.concatenate(
        [
            lax.dynamic_slice_in_dim(tokens, own, half, 1),
            lax.dynamic_slice_in_dim(cotangent, own, half, 1),
        ],
        axis=1,
    )
    is_cot = jnp.arange(width) >= half
    scale = jnp.where(is_cot[None, :], slot_gate[:, None], 1.0)
    sent = (mm(select, both) * scale).astype(BF16)
    got = to_each(sent.reshape(experts, cap, width)).reshape(slots, width)

    s_hidden, s_gate, s_up, _ = to_hidden(tokens, cotangent, sh_gate, sh_up, sh_down)
    hid = s_hidden.shape[1]
    s_both = jnp.concatenate([sh_gate, sh_up], axis=1)
    s_d = jnp.concatenate([s_gate, s_up], axis=1)
    s_other = input_rows(s_d, s_both, other, half)
    s_own = input_rows(s_d, s_both, own, half)
    side = coords(0)[1]
    grid = (side, side, side, width // experts, hid)
    terms_g = mm(tokens, s_gate, ROWS).astype(BF16).reshape(grid)
    terms_u = mm(tokens, s_up, ROWS).astype(BF16).reshape(grid)
    terms_d = mm(cotangent, s_hidden, ROWS).astype(BF16).reshape(grid)
    shared_g = summed_over(terms_g, (0, 1, 2))
    shared_u = summed_over(terms_u, (1, 2, 0))
    shared_d = summed_over(terms_d, (2, 0, 1))
    down_part = jnp.sum(shared_d * shared_d, axis=0)
    shared_d = shared_d.T
    s_peer = swap(s_other)
    w_gu = jnp.concatenate([w_g, w_u], axis=1)
    w_gu_own = lax.dynamic_slice_in_dim(w_gu, own, half, 0)
    w_gu_other = lax.dynamic_slice_in_dim(w_gu, other, half, 0)
    w_d_own = lax.dynamic_slice_in_dim(w_d, own, half, 1)
    w_d_other = lax.dynamic_slice_in_dim(w_d, other, half, 1)

    peer = swap(got)
    pre = mm(got[:, :half], w_gu_own) + mm(peer[:, :half], w_gu_other)
    hidden_cot = mm(got[:, half:], w_d_own, COLS) + mm(peer[:, half:], w_d_other, COLS)
    gate_pre, up_pre = pre[:, :hid], pre[:, hid:]
    active, slope = silu_parts(gate_pre)
    hidden = (active * up_pre).astype(BF16)
    gate_part = jnp.sum(hidden.astype(F32) * hidden_cot, axis=1)
    d_both = jnp.concatenate([hidden_cot * up_pre * slope, hidden_cot * active], axis=1).astype(BF16)
    rows_other = mm(d_both, w_gu_other, COLS).astype(BF16)
    rows_own = mm(d_both, w_gu_own, COLS).astype(BF16)
    from_peer = swap(rows_other)
    gate_peer = swap(gate_part)
    slot_rows = (from_peer.astype(F32) + rows_own.astype(F32)).astype(BF16)
    back_rows = to_each(slot_rows.reshape(experts, cap, half)).reshape(slots, half)

    low = tp == 0
    inputs = jnp.concatenate(
        [jnp.where(low, got[:, :half], peer[:, :half]), jnp.where(low, peer[:, :half], got[:, :half])],
        axis=1,
    )
    cots = jnp.concatenate(
        [jnp.where(low, got[:, half:], peer[:, half:]), jnp.where(low, peer[:, half:], got[:, half:])],
        axis=1,
    )
    grad_g = mm(inputs, d_both[:, :hid], ROWS)
    grad_u = mm(inputs, d_both[:, hid:], ROWS)
    grad_d = mm(hidden, cots, ROWS)

    s_rows = s_peer.astype(F32) + s_own.astype(F32)
    gate_sum = gate_part + gate_peer
    back_gate, down_norms = far_and_wide(gate_sum.reshape(experts, cap), down_part)

    norms = jnp.concatenate(
        [
            jnp.sum(grad_g * grad_g, axis=1),
            jnp.sum(grad_u * grad_u, axis=1),
            jnp.sum(shared_g * shared_g, axis=1),
            jnp.sum(shared_u * shared_u, axis=1),
        ]
    )
    norms = norms + swap(norms)
    step = width // experts
    gate_norms, up_norms = norms[:width], norms[width : 2 * width]
    shared_gate_norms, shared_up_norms = norms[2 * width : 2 * width + step], norms[2 * width + step :]

    routed = mm(select, back_rows, ROWS)
    token_grad = (routed + s_rows).astype(BF16)
    gate_at = jnp.sum(jnp.where(pick, back_gate[:, :, None], 0.0), axis=1)
    gate_grad = (
        jnp.stack([jnp.sum(jnp.where(name, gate_at, 0.0), axis=0) for name in names], axis=1) / gates
    )
    return (
        token_grad,
        gate_grad,
        grad_g[None],
        grad_u[None],
        grad_d[None],
        shared_g,
        shared_u,
        shared_d,
        gate_norms[None],
        up_norms[None],
        jnp.sum(grad_d * grad_d, axis=1)[None],
        shared_gate_norms,
        shared_up_norms,
        down_norms,
    )


def solution(mesh):
    placed = (
        P("ep", None),
        P("ep", None),
        P("ep", None),
        P("ep", None),
        P("ep", None, "tp"),
        P("ep", None, "tp"),
        P("ep", "tp", None),
        P(None, "tp"),
        P(None, "tp"),
        P("tp", None),
    )
    return jax.shard_map(
        layer,
        mesh=mesh,
        in_specs=placed,
        out_specs=(
            P("ep", "tp"),
            P("ep", None),
            P("ep", None, "tp"),
            P("ep", None, "tp"),
            P("ep", "tp", None),
            P("ep", "tp"),
            P("ep", "tp"),
            P("tp", "ep"),
            P("ep", None),
            P("ep", None),
            P("ep", "tp"),
            P("ep"),
            P("ep"),
            P("tp"),
        ),
        check_vma=False,
    )
```

```python
import jax
import jax.numpy as jnp
from jax import lax
from jax.experimental import pallas as pl
from jax.experimental.pallas import tpu as pltpu
from jax.sharding import PartitionSpec as P


F32 = jnp.float32
BF16 = jnp.bfloat16
ROWS = (((0,), (0,)), ((), ()))
COLS = (((1,), (1,)), ((), ()))
PLAIN = (((1,), (0,)), ((), ()))


def mm(a, b, contract=PLAIN):
    return lax.dot_general(a, b, contract, preferred_element_type=F32)


def swap(x):
    return lax.ppermute(x, "tp", [(0, 1), (1, 0)])


def to_each(x):
    return lax.all_to_all(x, "ep", 0, 0, tiled=True)


def routing_kernel(tp_ref, ids_ref, gates_ref, tok_ref, cot_ref, sent_ref, place_ref, place_at, gate_at):
    experts, tok_rows = place_at.shape
    rows, width = sent_ref.shape
    half = width // 2
    steps = pl.num_programs(0)
    block = experts // steps
    cap = rows // block
    step = pl.program_id(0)

    @pl.when(step == 0)
    def _():
        e = lax.broadcasted_iota(jnp.int32, (experts, tok_rows), 0)
        hit = jnp.zeros((experts, tok_rows), F32)
        gate_of = jnp.zeros((experts, tok_rows), F32)
        for k in range(ids_ref.shape[0]):
            name = ids_ref[k : k + 1, :] == e
            hit = jnp.where(name, 1.0, hit)
            gate_of = jnp.where(name, gates_ref[k : k + 1, :], gate_of)
        earlier = lax.broadcasted_iota(jnp.int32, (tok_rows, tok_rows), 0)
        later = lax.broadcasted_iota(jnp.int32, (tok_rows, tok_rows), 1)
        before = jnp.where(earlier < later, 1.0, 0.0).astype(BF16)
        rank = mm(hit.astype(BF16), before)
        place = jnp.where(hit > 0.0, rank, -1.0)
        place_at[...] = place
        gate_at[...] = gate_of
        place_ref[...] = place

    r = lax.broadcasted_iota(jnp.int32, (cap, tok_rows), 0).astype(F32)
    picks, scales = [], []
    for j in range(block):
        at = pl.ds(step * block + j, 1)
        pick = jnp.broadcast_to(place_at[at, :], (cap, tok_rows)) == r
        picks.append(jnp.where(pick, 1.0, 0.0))
        scales.append(jnp.sum(jnp.where(pick, gate_at[at, :], 0.0), axis=1, keepdims=True))
    select = jnp.concatenate(picks, axis=0).astype(BF16)
    scale = jnp.concatenate(scales, axis=0)
    sent_ref[:, :half] = mm(select, tok_ref[...]).astype(BF16)
    sent_ref[:, half:] = (mm(select, cot_ref[...]) * scale).astype(BF16)


def routing(tp, ids_t, gates_t, tokens, cotangent, experts, cap):
    tok_rows, width = tokens.shape
    half = width // 2
    top = ids_t.shape[0]
    steps = 8
    rows = experts * cap // steps
    return pl.pallas_call(
        routing_kernel,
        grid_spec=pltpu.PrefetchScalarGridSpec(
            num_scalar_prefetch=1,
            grid=(steps,),
            in_specs=[
                pl.BlockSpec((top, tok_rows), lambda i, tp: (0, 0)),
                pl.BlockSpec((top, tok_rows), lambda i, tp: (0, 0)),
                pl.BlockSpec((tok_rows, half), lambda i, tp: (0, tp[0])),
                pl.BlockSpec((tok_rows, half), lambda i, tp: (0, tp[0])),
            ],
            out_specs=[
                pl.BlockSpec((rows, width), lambda i, tp: (i, 0)),
                pl.BlockSpec((experts, tok_rows), lambda i, tp: (0, 0)),
            ],
            scratch_shapes=[pltpu.VMEM((experts, tok_rows), F32), pltpu.VMEM((experts, tok_rows), F32)],
        ),
        out_shape=[
            jax.ShapeDtypeStruct((experts * cap, width), BF16),
            jax.ShapeDtypeStruct((experts, tok_rows), F32),
        ],
        name="routing",
    )(tp.reshape(1), ids_t, gates_t, tokens, cotangent)


def payload_kernel(own_ref, peer_ref, out_ref):
    block, lines, lanes = out_ref.shape
    cap = own_ref.shape[0] // block
    for e in range(block):
        at = slice(e * cap, (e + 1) * cap)
        for c in range(lines // cap):
            cols = slice(c * lanes, (c + 1) * lanes)
            both = own_ref[at, cols].astype(F32) + peer_ref[at, cols].astype(F32)
            out_ref[e, c * cap : (c + 1) * cap, :] = both.astype(BF16)


def payload_of(own, peer, experts, extra):
    slots, half = own.shape
    steps = 8
    cap = slots // experts
    lines = cap * half // 128
    return pl.pallas_call(
        payload_kernel,
        grid=(steps,),
        in_specs=[pl.BlockSpec((slots // steps, half), lambda i: (i, 0))] * 2,
        out_specs=pl.BlockSpec((experts // steps, lines, 128), lambda i: (i, 0, 0)),
        out_shape=jax.ShapeDtypeStruct((experts, lines + extra, 128), BF16),
        name="payload",
    )(own, peer)


def total_kernel(got_ref, notes_ref, payload_ref, sums_ref, out_ref, acc):
    step = pl.program_id(0)
    part = jnp.sum(got_ref[...].astype(F32), axis=0)

    @pl.when(step == 0)
    def _():
        acc[...] = part

    @pl.when(step > 0)
    def _():
        acc[...] = acc[...] + part

    @pl.when(step == pl.num_programs(0) - 1)
    def _():
        total = acc[...]
        sums_ref[...] = total
        down = total[:, 2 * (total.shape[1] // 3) :]
        norms = jnp.sum(down * down, axis=0, keepdims=True)
        high = norms.astype(BF16).astype(F32)
        low = norms - high
        lines = out_ref.shape[1:]
        row = lax.broadcasted_iota(jnp.int32, lines, 0)
        marks = jnp.zeros(lines, F32)
        pieces = norms.shape[1] // lines[1]
        for at, value in enumerate((high, low)):
            for c in range(pieces):
                line = value[:, c * lines[1] : (c + 1) * lines[1]]
                marks = jnp.where(row == at * pieces + c, line, marks)
        out_ref[...] = (notes_ref[...] + marks[None]).astype(BF16)


def totals(got, notes, payload):
    size, rows, cols = got.shape
    steps = 4
    experts, extra, lanes = notes.shape
    last = payload.shape[1] // extra - 1
    return pl.pallas_call(
        total_kernel,
        grid=(steps,),
        in_specs=[
            pl.BlockSpec((size // steps, rows, cols), lambda i: (i, 0, 0)),
            pl.BlockSpec((experts, extra, lanes), lambda i: (0, 0, 0)),
            pl.BlockSpec(memory_space=pl.ANY),
        ],
        out_specs=[
            pl.BlockSpec((rows, cols), lambda i: (0, 0)),
            pl.BlockSpec((experts, extra, lanes), lambda i: (0, last, 0)),
        ],
        out_shape=[
            jax.ShapeDtypeStruct((rows, cols), F32),
            jax.ShapeDtypeStruct(payload.shape, BF16),
        ],
        input_output_aliases={2: 1},
        scratch_shapes=[pltpu.VMEM((rows, cols), F32)],
        name="totals",
    )(got, notes, payload)


def final_kernel(rows_ref, notes_ref, select_ref, own_ref, peer_ref, place_ref, ids_ref, gates_ref, tok_ref, gate_ref, down_ref):
    experts, lines, lanes = rows_ref.shape
    cap = lines // 2
    left = rows_ref[:, :cap, :].reshape(experts * cap, lanes)
    right = rows_ref[:, cap:, :].reshape(experts * cap, lanes)
    back = jnp.concatenate([left, right], axis=1)
    routed = mm(select_ref[...], back)
    tok_ref[...] = (routed + (own_ref[...].astype(F32) + peer_ref[...].astype(F32))).astype(BF16)

    @pl.when(pl.program_id(0) == 0)
    def _():
        notes = notes_ref[...].astype(F32)
        whole = jnp.sum(notes, axis=0)
        down_ref[...] = whole
        row = lax.broadcasted_iota(jnp.int32, notes.shape, 1)
        gate = jnp.sum(jnp.where((row == 4) | (row == 5), notes, 0.0), axis=1)
        place = place_ref[...]
        at = jnp.zeros(place.shape, F32)
        for r in range(cap):
            at = jnp.where(place == r, gate[:, r : r + 1], at)
        e = lax.broadcasted_iota(jnp.int32, place.shape, 0)
        for k in range(ids_ref.shape[0]):
            mine = jnp.sum(jnp.where(ids_ref[k : k + 1, :] == e, at, 0.0), axis=0, keepdims=True)
            gate_ref[k : k + 1, :] = mine / gates_ref[k : k + 1, :]


def finished(payload, select_t, s_own, s_peer, place, ids_t, gates_t):
    experts, lines, lanes = payload.shape
    tok_rows, half = s_own.shape
    slots = select_t.shape[1]
    cap = slots // experts
    steps = half // (2 * lanes)
    extra = lines - cap * half // lanes
    return pl.pallas_call(
        final_kernel,
        grid=(steps,),
        in_specs=[
            pl.BlockSpec((experts, 2 * cap, lanes), lambda i: (0, i, 0)),
            pl.BlockSpec((experts, extra, lanes), lambda i: (0, lines // extra - 1, 0)),
            pl.BlockSpec((tok_rows, slots), lambda i: (0, 0)),
            pl.BlockSpec((tok_rows, 2 * lanes), lambda i: (0, i)),
            pl.BlockSpec((tok_rows, 2 * lanes), lambda i: (0, i)),
            pl.BlockSpec(place.shape, lambda i: (0, 0)),
            pl.BlockSpec(ids_t.shape, lambda i: (0, 0)),
            pl.BlockSpec(gates_t.shape, lambda i: (0, 0)),
        ],
        out_specs=[
            pl.BlockSpec((tok_rows, 2 * lanes), lambda i: (0, i)),
            pl.BlockSpec(gates_t.shape, lambda i: (0, 0)),
            pl.BlockSpec((extra, lanes), lambda i: (0, 0)),
        ],
        out_shape=[
            jax.ShapeDtypeStruct((tok_rows, half), BF16),
            jax.ShapeDtypeStruct(gates_t.shape, F32),
            jax.ShapeDtypeStruct((extra, lanes), F32),
        ],
        name="final",
    )(payload, payload, select_t, s_own, s_peer, place, ids_t, gates_t)


def silu_parts(pre):
    sigmoid = jax.nn.sigmoid(pre)
    return (pre * sigmoid, sigmoid * (1.0 + pre * (1.0 - sigmoid)))


def to_hidden(inputs, cots, w_g, w_u, w_d):
    gate_pre = mm(inputs, w_g)
    up_pre = mm(inputs, w_u)
    active, slope = silu_parts(gate_pre)
    hidden = (active * up_pre).astype(BF16)
    hidden_cot = mm(cots, w_d, COLS)
    gate_part = jnp.sum(hidden.astype(F32) * hidden_cot, axis=1)
    d_gate = (hidden_cot * up_pre * slope).astype(BF16)
    d_up = (hidden_cot * active).astype(BF16)
    return hidden, d_gate, d_up, gate_part


def input_rows(d_both, w_both, first, width):
    return mm(d_both, lax.dynamic_slice_in_dim(w_both, first, width, 0), COLS).astype(BF16)


def layer(tokens, expert_ids, gates, cotangent, w_gate, w_up, w_down, sh_gate, sh_up, sh_down):
    experts = lax.axis_size("ep")
    tok_rows, width = tokens.shape
    top = expert_ids.shape[1]
    cap = 3 * tok_rows * top // (2 * experts)
    slots = experts * cap
    half = width // 2
    tp = lax.axis_index("tp")
    own, other = tp * half, (1 - tp) * half
    w_g, w_u, w_d = w_gate[0], w_up[0], w_down[0]

    ids_t = expert_ids.T
    gates_t = gates.T
    sent, place = routing(tp, ids_t, gates_t, tokens, cotangent, experts, cap)
    got = to_each(sent.reshape(experts, cap, width)).reshape(slots, width)

    s_hidden, s_gate, s_up, _ = to_hidden(tokens, cotangent, sh_gate, sh_up, sh_down)
    hid = s_hidden.shape[1]
    s_both = jnp.concatenate([sh_gate, sh_up], axis=1)
    s_d = jnp.concatenate([s_gate, s_up], axis=1)
    s_other = input_rows(s_d, s_both, other, half)
    s_own = input_rows(s_d, s_both, own, half)
    shared = jnp.concatenate([mm(tokens, s_d, ROWS), mm(cotangent, s_hidden, ROWS)], axis=1).astype(BF16)
    shared_got = to_each(shared.reshape(experts, width // experts, 3 * hid))
    s_peer = swap(s_other)
    w_gu = jnp.concatenate([w_g, w_u], axis=1)
    w_gu_own = lax.dynamic_slice_in_dim(w_gu, own, half, 0)
    w_gu_other = lax.dynamic_slice_in_dim(w_gu, other, half, 0)
    w_d_own = lax.dynamic_slice_in_dim(w_d, own, half, 1)
    w_d_other = lax.dynamic_slice_in_dim(w_d, other, half, 1)

    slot = jnp.arange(slots, dtype=jnp.int32)
    pick = place.T[:, :, None] == (slot[:cap].astype(F32))[None, None, :]
    select_t = pick.astype(BF16).reshape(tok_rows, slots)
    peer = swap(got)
    pre = mm(got[:, :half], w_gu_own) + mm(peer[:, :half], w_gu_other)
    hidden_cot = mm(got[:, half:], w_d_own, COLS) + mm(peer[:, half:], w_d_other, COLS)
    gate_pre, up_pre = pre[:, :hid], pre[:, hid:]
    active, slope = silu_parts(gate_pre)
    hidden = (active * up_pre).astype(BF16)
    gate_part = jnp.sum(hidden.astype(F32) * hidden_cot, axis=1)
    d_both = jnp.concatenate([hidden_cot * up_pre * slope, hidden_cot * active], axis=1).astype(BF16)
    rows_other = mm(d_both, w_gu_other, COLS).astype(BF16)
    rows_own = mm(d_both, w_gu_own, COLS).astype(BF16)
    from_peer = swap(rows_other)
    gate_peer = swap(gate_part)
    extra = 8
    payload = payload_of(rows_own, from_peer, experts, extra)
    gate_sum = jnp.pad((gate_part + gate_peer).reshape(experts, 1, cap), ((0, 0), (0, 0), (0, 128 - cap)))
    high = lax.reduce_precision(gate_sum, 8, 7)
    line = jnp.arange(extra)[None, :, None]
    notes = jnp.where(line == 4, high, jnp.where(line == 5, gate_sum - high, 0.0))
    shared_sum, payload = totals(shared_got, notes, payload)
    back = to_each(payload)
    shared_g, shared_u = shared_sum[:, :hid], shared_sum[:, hid : 2 * hid]
    shared_d = shared_sum[:, 2 * hid :].T

    low = tp == 0
    inputs = jnp.concatenate(
        [jnp.where(low, got[:, :half], peer[:, :half]), jnp.where(low, peer[:, :half], got[:, :half])],
        axis=1,
    )
    cots = jnp.concatenate(
        [jnp.where(low, got[:, half:], peer[:, half:]), jnp.where(low, peer[:, half:], got[:, half:])],
        axis=1,
    )
    grad_g = mm(inputs, d_both[:, :hid], ROWS)
    grad_u = mm(inputs, d_both[:, hid:], ROWS)
    grad_d = mm(hidden, cots, ROWS)

    norms = jnp.concatenate(
        [
            jnp.sum(grad_g * grad_g, axis=1),
            jnp.sum(grad_u * grad_u, axis=1),
            jnp.sum(shared_g * shared_g, axis=1),
            jnp.sum(shared_u * shared_u, axis=1),
        ]
    )
    norms = norms + swap(norms)
    step = width // experts
    gate_norms, up_norms = norms[:width], norms[width : 2 * width]
    shared_gate_norms, shared_up_norms = norms[2 * width : 2 * width + step], norms[2 * width + step :]

    token_grad, gate_grad, whole = finished(back, select_t, s_own, s_peer, place, ids_t, gates_t)
    gate_grad = gate_grad.T
    lines = hid // 128
    down_norms = (whole[:lines] + whole[lines : 2 * lines]).reshape(hid)
    return (
        token_grad,
        gate_grad,
        grad_g[None],
        grad_u[None],
        grad_d[None],
        shared_g,
        shared_u,
        shared_d,
        gate_norms[None],
        up_norms[None],
        jnp.sum(grad_d * grad_d, axis=1)[None],
        shared_gate_norms,
        shared_up_norms,
        down_norms,
    )


def solution(mesh):
    placed = (
        P("ep", None),
        P("ep", None),
        P("ep", None),
        P("ep", None),
        P("ep", None, "tp"),
        P("ep", None, "tp"),
        P("ep", "tp", None),
        P(None, "tp"),
        P(None, "tp"),
        P("tp", None),
    )
    return jax.shard_map(
        layer,
        mesh=mesh,
        in_specs=placed,
        out_specs=(
            P("ep", "tp"),
            P("ep", None),
            P("ep", None, "tp"),
            P("ep", None, "tp"),
            P("ep", "tp", None),
            P("ep", "tp"),
            P("ep", "tp"),
            P("tp", "ep"),
            P("ep", None),
            P("ep", None),
            P("ep", "tp"),
            P("ep"),
            P("ep"),
            P("tp"),
        ),
        check_vma=False,
    )
```

```python
import jax
import jax.numpy as jnp
from jax import lax
from jax.experimental import pallas as pl
from jax.experimental.pallas import tpu as pltpu
from jax.sharding import PartitionSpec as P


F32 = jnp.float32
BF16 = jnp.bfloat16
ROWS = (((0,), (0,)), ((), ()))
COLS = (((1,), (1,)), ((), ()))
PLAIN = (((1,), (0,)), ((), ()))
SIDE = 4


def mm(a, b, contract=PLAIN):
    return lax.dot_general(a, b, contract, preferred_element_type=F32)


def swap(x):
    return lax.ppermute(x, "tp", [(0, 1), (1, 0)])


def to_each(x):
    return lax.all_to_all(x, "ep", 0, 0, tiled=True)


def routing_kernel(tp_ref, ids_ref, gates_ref, tok_ref, cot_ref, sent_ref, place_ref, place_at, gate_at):
    experts, tok_rows = place_at.shape
    rows, width = sent_ref.shape
    half = width // 2
    steps = pl.num_programs(0)
    block = experts // steps
    cap = rows // block
    step = pl.program_id(0)

    @pl.when(step == 0)
    def _():
        e = lax.broadcasted_iota(jnp.int32, (experts, tok_rows), 0)
        hit = jnp.zeros((experts, tok_rows), F32)
        gate_of = jnp.zeros((experts, tok_rows), F32)
        for k in range(ids_ref.shape[0]):
            name = ids_ref[k : k + 1, :] == e
            hit = jnp.where(name, 1.0, hit)
            gate_of = jnp.where(name, gates_ref[k : k + 1, :], gate_of)
        earlier = lax.broadcasted_iota(jnp.int32, (tok_rows, tok_rows), 0)
        later = lax.broadcasted_iota(jnp.int32, (tok_rows, tok_rows), 1)
        before = jnp.where(earlier < later, 1.0, 0.0).astype(BF16)
        rank = mm(hit.astype(BF16), before)
        place = jnp.where(hit > 0.0, rank, -1.0)
        place_at[...] = place
        gate_at[...] = gate_of
        place_ref[...] = place

    r = lax.broadcasted_iota(jnp.int32, (cap, tok_rows), 0).astype(F32)
    picks, scales = [], []
    for j in range(block):
        at = pl.ds(step * block + j, 1)
        pick = jnp.broadcast_to(place_at[at, :], (cap, tok_rows)) == r
        picks.append(jnp.where(pick, 1.0, 0.0))
        scales.append(jnp.sum(jnp.where(pick, gate_at[at, :], 0.0), axis=1, keepdims=True))
    select = jnp.concatenate(picks, axis=0).astype(BF16)
    scale = jnp.concatenate(scales, axis=0)
    sent_ref[:, :half] = mm(select, tok_ref[...]).astype(BF16)
    sent_ref[:, half:] = (mm(select, cot_ref[...]) * scale).astype(BF16)


def routing(tp, ids_t, gates_t, tokens, cotangent, experts, cap):
    tok_rows, width = tokens.shape
    half = width // 2
    top = ids_t.shape[0]
    steps = 4
    rows = experts * cap // steps
    return pl.pallas_call(
        routing_kernel,
        grid_spec=pltpu.PrefetchScalarGridSpec(
            num_scalar_prefetch=1,
            grid=(steps,),
            in_specs=[
                pl.BlockSpec((top, tok_rows), lambda i, tp: (0, 0)),
                pl.BlockSpec((top, tok_rows), lambda i, tp: (0, 0)),
                pl.BlockSpec((tok_rows, half), lambda i, tp: (0, tp[0])),
                pl.BlockSpec((tok_rows, half), lambda i, tp: (0, tp[0])),
            ],
            out_specs=[
                pl.BlockSpec((rows, width), lambda i, tp: (i, 0)),
                pl.BlockSpec((experts, tok_rows), lambda i, tp: (0, 0)),
            ],
            scratch_shapes=[pltpu.VMEM((experts, tok_rows), F32), pltpu.VMEM((experts, tok_rows), F32)],
        ),
        out_shape=[
            jax.ShapeDtypeStruct((experts * cap, width), BF16),
            jax.ShapeDtypeStruct((experts, tok_rows), F32),
        ],
        name="routing",
    )(tp.reshape(1), ids_t, gates_t, tokens, cotangent)


def payload_kernel(own_ref, peer_ref, out_ref):
    block, lines, lanes = out_ref.shape
    cap = own_ref.shape[0] // block
    for e in range(block):
        at = slice(e * cap, (e + 1) * cap)
        for c in range(lines // cap):
            cols = slice(c * lanes, (c + 1) * lanes)
            both = own_ref[at, cols].astype(F32) + peer_ref[at, cols].astype(F32)
            out_ref[e, c * cap : (c + 1) * cap, :] = both.astype(BF16)


def payload_of(own, peer, experts, extra):
    slots, half = own.shape
    steps = 8
    cap = slots // experts
    lines = cap * half // 128
    return pl.pallas_call(
        payload_kernel,
        grid=(steps,),
        in_specs=[pl.BlockSpec((slots // steps, half), lambda i: (i, 0))] * 2,
        out_specs=pl.BlockSpec((experts // steps, lines, 128), lambda i: (i, 0, 0)),
        out_shape=jax.ShapeDtypeStruct((experts, lines + extra, 128), BF16),
        name="payload",
    )(own, peer)


def total_kernel(got_ref, notes_ref, payload_ref, sums_ref, out_ref, acc):
    step = pl.program_id(0)
    part = jnp.sum(got_ref[...].astype(F32), axis=0)

    @pl.when(step == 0)
    def _():
        acc[...] = part

    @pl.when(step > 0)
    def _():
        acc[...] = acc[...] + part

    @pl.when(step == pl.num_programs(0) - 1)
    def _():
        total = acc[...]
        sums_ref[...] = total
        down = total[:, 2 * (total.shape[1] // 3) :]
        norms = jnp.sum(down * down, axis=0, keepdims=True)
        high = norms.astype(BF16).astype(F32)
        low = norms - high
        lines = out_ref.shape[1:]
        row = lax.broadcasted_iota(jnp.int32, lines, 0)
        marks = jnp.zeros(lines, F32)
        pieces = norms.shape[1] // lines[1]
        for at, value in enumerate((high, low)):
            for c in range(pieces):
                line = value[:, c * lines[1] : (c + 1) * lines[1]]
                marks = jnp.where(row == at * pieces + c, line, marks)
        out_ref[...] = (notes_ref[...] + marks[None]).astype(BF16)


def totals(got, notes, payload):
    size, rows, cols = got.shape
    steps = 2
    experts, extra, lanes = notes.shape
    last = payload.shape[1] // extra - 1
    return pl.pallas_call(
        total_kernel,
        grid=(steps,),
        in_specs=[
            pl.BlockSpec((size // steps, rows, cols), lambda i: (i, 0, 0)),
            pl.BlockSpec((experts, extra, lanes), lambda i: (0, 0, 0)),
            pl.BlockSpec(memory_space=pl.ANY),
        ],
        out_specs=[
            pl.BlockSpec((rows, cols), lambda i: (0, 0)),
            pl.BlockSpec((experts, extra, lanes), lambda i: (0, last, 0)),
        ],
        out_shape=[
            jax.ShapeDtypeStruct((rows, cols), F32),
            jax.ShapeDtypeStruct(payload.shape, BF16),
        ],
        input_output_aliases={2: 1},
        scratch_shapes=[pltpu.VMEM((rows, cols), F32)],
        name="totals",
    )(got, notes, payload)


def final_kernel(rows_ref, notes_ref, select_ref, own_ref, peer_ref, place_ref, ids_ref, gates_ref, tok_ref, gate_ref, down_ref):
    experts, lines, lanes = rows_ref.shape
    cap = lines // 2
    left = rows_ref[:, :cap, :].reshape(experts * cap, lanes)
    right = rows_ref[:, cap:, :].reshape(experts * cap, lanes)
    back = jnp.concatenate([left, right], axis=1)
    routed = mm(select_ref[...], back)
    tok_ref[...] = (routed + (own_ref[...].astype(F32) + peer_ref[...].astype(F32))).astype(BF16)

    @pl.when(pl.program_id(0) == 0)
    def _():
        notes = notes_ref[...].astype(F32)
        whole = jnp.sum(notes, axis=0)
        down_ref[...] = jnp.concatenate([whole[0:1] + whole[2:3], whole[1:2] + whole[3:4]], axis=1)
        row = lax.broadcasted_iota(jnp.int32, notes.shape, 1)
        gate = jnp.sum(jnp.where((row == 4) | (row == 5), notes, 0.0), axis=1)
        place = place_ref[...]
        at = jnp.zeros(place.shape, F32)
        for r in range(cap):
            at = jnp.where(place == r, gate[:, r : r + 1], at)
        e = lax.broadcasted_iota(jnp.int32, place.shape, 0)
        for k in range(ids_ref.shape[0]):
            mine = jnp.sum(jnp.where(ids_ref[k : k + 1, :] == e, at, 0.0), axis=0, keepdims=True)
            gate_ref[k : k + 1, :] = mine / gates_ref[k : k + 1, :]


def finished(payload, select_t, s_own, s_peer, place, ids_t, gates_t):
    experts, lines, lanes = payload.shape
    tok_rows, half = s_own.shape
    slots = select_t.shape[1]
    cap = slots // experts
    steps = half // (2 * lanes)
    extra = lines - cap * half // lanes
    return pl.pallas_call(
        final_kernel,
        grid=(steps,),
        in_specs=[
            pl.BlockSpec((experts, 2 * cap, lanes), lambda i: (0, i, 0)),
            pl.BlockSpec((experts, extra, lanes), lambda i: (0, lines // extra - 1, 0)),
            pl.BlockSpec((tok_rows, slots), lambda i: (0, 0)),
            pl.BlockSpec((tok_rows, 2 * lanes), lambda i: (0, i)),
            pl.BlockSpec((tok_rows, 2 * lanes), lambda i: (0, i)),
            pl.BlockSpec(place.shape, lambda i: (0, 0)),
            pl.BlockSpec(ids_t.shape, lambda i: (0, 0)),
            pl.BlockSpec(gates_t.shape, lambda i: (0, 0)),
        ],
        out_specs=[
            pl.BlockSpec((tok_rows, 2 * lanes), lambda i: (0, i)),
            pl.BlockSpec(gates_t.shape, lambda i: (0, 0)),
            pl.BlockSpec((1, 2 * lanes), lambda i: (0, 0)),
        ],
        out_shape=[
            jax.ShapeDtypeStruct((tok_rows, half), BF16),
            jax.ShapeDtypeStruct(gates_t.shape, F32),
            jax.ShapeDtypeStruct((1, 2 * lanes), F32),
        ],
        name="final",
    )(payload, payload, select_t, s_own, s_peer, place, ids_t, gates_t)


def next_along(x, by):
    size = lax.axis_size("ep")
    return lax.ppermute(x, "ep", [(i, (i + by * (size // SIDE)) % size) for i in range(size)])


def silu_parts(pre):
    sigmoid = jax.nn.sigmoid(pre)
    return (pre * sigmoid, sigmoid * (1.0 + pre * (1.0 - sigmoid)))


def to_hidden(inputs, cots, w_g, w_u, w_d):
    gate_pre = mm(inputs, w_g)
    up_pre = mm(inputs, w_u)
    active, slope = silu_parts(gate_pre)
    hidden = (active * up_pre).astype(BF16)
    hidden_cot = mm(cots, w_d, COLS)
    gate_part = jnp.sum(hidden.astype(F32) * hidden_cot, axis=1)
    d_gate = (hidden_cot * up_pre * slope).astype(BF16)
    d_up = (hidden_cot * active).astype(BF16)
    return hidden, d_gate, d_up, gate_part


def input_rows(d_both, w_both, first, width):
    return mm(d_both, lax.dynamic_slice_in_dim(w_both, first, width, 0), COLS).astype(BF16)


def layer(tokens, expert_ids, gates, cotangent, w_gate, w_up, w_down, sh_gate, sh_up, sh_down):
    experts = lax.axis_size("ep")
    tok_rows, width = tokens.shape
    top = expert_ids.shape[1]
    cap = 3 * tok_rows * top // (2 * experts)
    slots = experts * cap
    half = width // 2
    tp = lax.axis_index("tp")
    own, other = tp * half, (1 - tp) * half
    w_g, w_u, w_d = w_gate[0], w_up[0], w_down[0]

    ids_t = expert_ids.T
    gates_t = gates.T
    sent, place = routing(tp, ids_t, gates_t, tokens, cotangent, experts, cap)
    got = to_each(sent.reshape(experts, cap, width)).reshape(slots, width)

    s_hidden, s_gate, s_up, _ = to_hidden(tokens, cotangent, sh_gate, sh_up, sh_down)
    hid = s_hidden.shape[1]
    s_both = jnp.concatenate([sh_gate, sh_up], axis=1)
    s_d = jnp.concatenate([s_gate, s_up], axis=1)
    s_other = input_rows(s_d, s_both, other, half)
    s_own = input_rows(s_d, s_both, own, half)
    shared = jnp.concatenate([mm(tokens, s_d, ROWS), mm(cotangent, s_hidden, ROWS)], axis=1).astype(BF16)
    plane = experts // SIDE
    z = lax.div(lax.axis_index("ep"), plane)
    part = width // SIDE
    pieces = [
        lax.dynamic_slice_in_dim(shared, lax.rem(z + by, SIDE) * part, part, 0) for by in range(SIDE)
    ]
    arrived = [next_along(pieces[by], by) for by in range(1, SIDE)]
    terms = pieces[0].astype(F32)
    for piece in arrived:
        terms = terms + piece.astype(F32)
    terms = terms.astype(BF16).reshape(plane, width // experts, 3 * hid)
    groups = [list(range(i, i + plane)) for i in range(0, experts, plane)]
    shared_got = lax.all_to_all(terms, "ep", 0, 0, tiled=True, axis_index_groups=groups)
    s_peer = swap(s_other)
    w_gu = jnp.concatenate([w_g, w_u], axis=1)
    w_gu_own = lax.dynamic_slice_in_dim(w_gu, own, half, 0)
    w_gu_other = lax.dynamic_slice_in_dim(w_gu, other, half, 0)
    w_d_own = lax.dynamic_slice_in_dim(w_d, own, half, 1)
    w_d_other = lax.dynamic_slice_in_dim(w_d, other, half, 1)

    slot = jnp.arange(slots, dtype=jnp.int32)
    pick = place.T[:, :, None] == (slot[:cap].astype(F32))[None, None, :]
    select_t = pick.astype(BF16).reshape(tok_rows, slots)
    peer = swap(got)
    pre = mm(got[:, :half], w_gu_own) + mm(peer[:, :half], w_gu_other)
    hidden_cot = mm(got[:, half:], w_d_own, COLS) + mm(peer[:, half:], w_d_other, COLS)
    gate_pre, up_pre = pre[:, :hid], pre[:, hid:]
    active, slope = silu_parts(gate_pre)
    hidden = (active * up_pre).astype(BF16)
    gate_part = jnp.sum(hidden.astype(F32) * hidden_cot, axis=1)
    d_both = jnp.concatenate([hidden_cot * up_pre * slope, hidden_cot * active], axis=1).astype(BF16)
    rows_other = mm(d_both, w_gu_other, COLS).astype(BF16)
    rows_own = mm(d_both, w_gu_own, COLS).astype(BF16)
    from_peer = swap(rows_other)
    gate_peer = swap(gate_part)
    extra = 8
    payload = payload_of(rows_own, from_peer, experts, extra)
    gate_sum = jnp.pad((gate_part + gate_peer).reshape(experts, 1, cap), ((0, 0), (0, 0), (0, 128 - cap)))
    high = lax.reduce_precision(gate_sum, 8, 7)
    line = jnp.arange(extra)[None, :, None]
    notes = jnp.where(line == 4, high, jnp.where(line == 5, gate_sum - high, 0.0))
    shared_sum, payload = totals(shared_got, notes, payload)
    back = to_each(payload)
    shared_g, shared_u = shared_sum[:, :hid], shared_sum[:, hid : 2 * hid]
    shared_d = shared_sum[:, 2 * hid :].T

    low = tp == 0
    inputs = jnp.concatenate(
        [jnp.where(low, got[:, :half], peer[:, :half]), jnp.where(low, peer[:, :half], got[:, :half])],
        axis=1,
    )
    cots = jnp.concatenate(
        [jnp.where(low, got[:, half:], peer[:, half:]), jnp.where(low, peer[:, half:], got[:, half:])],
        axis=1,
    )
    grad_g = mm(inputs, d_both[:, :hid], ROWS)
    grad_u = mm(inputs, d_both[:, hid:], ROWS)
    grad_d = mm(hidden, cots, ROWS)

    norms = jnp.concatenate(
        [
            jnp.sum(grad_g * grad_g, axis=1),
            jnp.sum(grad_u * grad_u, axis=1),
            jnp.sum(shared_g * shared_g, axis=1),
            jnp.sum(shared_u * shared_u, axis=1),
        ]
    )
    norms = norms + swap(norms)
    step = width // experts
    gate_norms, up_norms = norms[:width], norms[width : 2 * width]
    shared_gate_norms, shared_up_norms = norms[2 * width : 2 * width + step], norms[2 * width + step :]

    token_grad, gate_grad, down_norms = finished(back, select_t, s_own, s_peer, place, ids_t, gates_t)
    gate_grad = gate_grad.T
    down_norms = down_norms.reshape(hid)
    return (
        token_grad,
        gate_grad,
        grad_g[None],
        grad_u[None],
        grad_d[None],
        shared_g,
        shared_u,
        shared_d,
        gate_norms[None],
        up_norms[None],
        jnp.sum(grad_d * grad_d, axis=1)[None],
        shared_gate_norms,
        shared_up_norms,
        down_norms,
    )


def solution(mesh):
    placed = (
        P("ep", None),
        P("ep", None),
        P("ep", None),
        P("ep", None),
        P("ep", None, "tp"),
        P("ep", None, "tp"),
        P("ep", "tp", None),
        P(None, "tp"),
        P(None, "tp"),
        P("tp", None),
    )
    return jax.shard_map(
        layer,
        mesh=mesh,
        in_specs=placed,
        out_specs=(
            P("ep", "tp"),
            P("ep", None),
            P("ep", None, "tp"),
            P("ep", None, "tp"),
            P("ep", "tp", None),
            P("ep", "tp"),
            P("ep", "tp"),
            P("tp", "ep"),
            P("ep", None),
            P("ep", None),
            P("ep", "tp"),
            P("ep"),
            P("ep"),
            P("tp"),
        ),
        check_vma=False,
    )
```

```python
import jax
import jax.numpy as jnp
from jax import lax
from jax.experimental import pallas as pl
from jax.experimental.pallas import tpu as pltpu
from jax.sharding import PartitionSpec as P


F32 = jnp.float32
BF16 = jnp.bfloat16
ROWS = (((0,), (0,)), ((), ()))
COLS = (((1,), (1,)), ((), ()))
PLAIN = (((1,), (0,)), ((), ()))
SIDE = 4


def mm(a, b, contract=PLAIN):
    return lax.dot_general(a, b, contract, preferred_element_type=F32)


def swap(x):
    return lax.ppermute(x, "tp", [(0, 1), (1, 0)])


def to_each(x):
    return lax.all_to_all(x, "ep", 0, 0, tiled=True)


def routing_kernel(tp_ref, ids_ref, gates_ref, tok_ref, cot_ref, sent_ref, place_ref, place_at, gate_at):
    experts, tok_rows = place_at.shape
    rows, width = sent_ref.shape
    half = width // 2
    steps = pl.num_programs(0)
    block = experts // steps
    cap = rows // block
    step = pl.program_id(0)

    @pl.when(step == 0)
    def _():
        e = lax.broadcasted_iota(jnp.int32, (experts, tok_rows), 0)
        hit = jnp.zeros((experts, tok_rows), F32)
        gate_of = jnp.zeros((experts, tok_rows), F32)
        for k in range(ids_ref.shape[0]):
            name = ids_ref[k : k + 1, :] == e
            hit = jnp.where(name, 1.0, hit)
            gate_of = jnp.where(name, gates_ref[k : k + 1, :], gate_of)
        earlier = lax.broadcasted_iota(jnp.int32, (tok_rows, tok_rows), 0)
        later = lax.broadcasted_iota(jnp.int32, (tok_rows, tok_rows), 1)
        before = jnp.where(earlier < later, 1.0, 0.0).astype(BF16)
        rank = mm(hit.astype(BF16), before)
        place = jnp.where(hit > 0.0, rank, -1.0)
        place_at[...] = place
        gate_at[...] = gate_of
        place_ref[...] = place

    r = lax.broadcasted_iota(jnp.int32, (cap, tok_rows), 0).astype(F32)
    picks, scales = [], []
    for j in range(block):
        at = pl.ds(step * block + j, 1)
        pick = jnp.broadcast_to(place_at[at, :], (cap, tok_rows)) == r
        picks.append(jnp.where(pick, 1.0, 0.0))
        scales.append(jnp.sum(jnp.where(pick, gate_at[at, :], 0.0), axis=1, keepdims=True))
    select = jnp.concatenate(picks, axis=0).astype(BF16)
    scale = jnp.concatenate(scales, axis=0)
    sent_ref[:, :half] = mm(select, tok_ref[...]).astype(BF16)
    sent_ref[:, half:] = (mm(select, cot_ref[...]) * scale).astype(BF16)


def routing(tp, ids_t, gates_t, tokens, cotangent, experts, cap):
    tok_rows, width = tokens.shape
    half = width // 2
    top = ids_t.shape[0]
    steps = 4
    rows = experts * cap // steps
    return pl.pallas_call(
        routing_kernel,
        grid_spec=pltpu.PrefetchScalarGridSpec(
            num_scalar_prefetch=1,
            grid=(steps,),
            in_specs=[
                pl.BlockSpec((top, tok_rows), lambda i, tp: (0, 0)),
                pl.BlockSpec((top, tok_rows), lambda i, tp: (0, 0)),
                pl.BlockSpec((tok_rows, half), lambda i, tp: (0, tp[0])),
                pl.BlockSpec((tok_rows, half), lambda i, tp: (0, tp[0])),
            ],
            out_specs=[
                pl.BlockSpec((rows, width), lambda i, tp: (i, 0)),
                pl.BlockSpec((experts, tok_rows), lambda i, tp: (0, 0)),
            ],
            scratch_shapes=[pltpu.VMEM((experts, tok_rows), F32), pltpu.VMEM((experts, tok_rows), F32)],
        ),
        out_shape=[
            jax.ShapeDtypeStruct((experts * cap, width), BF16),
            jax.ShapeDtypeStruct((experts, tok_rows), F32),
        ],
        name="routing",
    )(tp.reshape(1), ids_t, gates_t, tokens, cotangent)


def payload_kernel(own_ref, peer_ref, out_ref):
    block, lines, lanes = out_ref.shape
    cap = own_ref.shape[0] // block
    for e in range(block):
        at = slice(e * cap, (e + 1) * cap)
        for c in range(lines // cap):
            cols = slice(c * lanes, (c + 1) * lanes)
            both = own_ref[at, cols].astype(F32) + peer_ref[at, cols].astype(F32)
            out_ref[e, c * cap : (c + 1) * cap, :] = both.astype(BF16)


def payload_of(own, peer, experts, extra):
    slots, half = own.shape
    steps = 8
    cap = slots // experts
    lines = cap * half // 128
    return pl.pallas_call(
        payload_kernel,
        grid=(steps,),
        in_specs=[pl.BlockSpec((slots // steps, half), lambda i: (i, 0))] * 2,
        out_specs=pl.BlockSpec((experts // steps, lines, 128), lambda i: (i, 0, 0)),
        out_shape=jax.ShapeDtypeStruct((experts, lines + extra, 128), BF16),
        name="payload",
    )(own, peer)


def total_kernel(got_ref, notes_ref, payload_ref, sums_ref, out_ref, acc):
    step = pl.program_id(0)
    part = jnp.sum(got_ref[...].astype(F32), axis=0)

    @pl.when(step == 0)
    def _():
        acc[...] = part

    @pl.when(step > 0)
    def _():
        acc[...] = acc[...] + part

    @pl.when(step == pl.num_programs(0) - 1)
    def _():
        total = acc[...]
        sums_ref[...] = total
        down = total[:, 2 * (total.shape[1] // 3) :]
        norms = jnp.sum(down * down, axis=0, keepdims=True)
        high = norms.astype(BF16).astype(F32)
        low = norms - high
        lines = out_ref.shape[1:]
        row = lax.broadcasted_iota(jnp.int32, lines, 0)
        marks = jnp.zeros(lines, F32)
        pieces = norms.shape[1] // lines[1]
        for at, value in enumerate((high, low)):
            for c in range(pieces):
                line = value[:, c * lines[1] : (c + 1) * lines[1]]
                marks = jnp.where(row == at * pieces + c, line, marks)
        out_ref[...] = (notes_ref[...] + marks[None]).astype(BF16)


def totals(got, notes, payload):
    size, rows, cols = got.shape
    steps = 2
    experts, extra, lanes = notes.shape
    last = payload.shape[1] // extra - 1
    return pl.pallas_call(
        total_kernel,
        grid=(steps,),
        in_specs=[
            pl.BlockSpec((size // steps, rows, cols), lambda i: (i, 0, 0)),
            pl.BlockSpec((experts, extra, lanes), lambda i: (0, 0, 0)),
            pl.BlockSpec(memory_space=pl.ANY),
        ],
        out_specs=[
            pl.BlockSpec((rows, cols), lambda i: (0, 0)),
            pl.BlockSpec((experts, extra, lanes), lambda i: (0, last, 0)),
        ],
        out_shape=[
            jax.ShapeDtypeStruct((rows, cols), F32),
            jax.ShapeDtypeStruct(payload.shape, BF16),
        ],
        input_output_aliases={2: 1},
        scratch_shapes=[pltpu.VMEM((rows, cols), F32)],
        name="totals",
    )(got, notes, payload)


def final_kernel(rows_ref, notes_ref, select_ref, own_ref, peer_ref, place_ref, ids_ref, gates_ref, tok_ref, gate_ref, down_ref, gate_at):
    experts, lines, lanes = rows_ref.shape
    cap = lines // 2
    left = rows_ref[:, :cap, :].reshape(experts * cap, lanes)
    right = rows_ref[:, cap:, :].reshape(experts * cap, lanes)
    back = jnp.concatenate([left, right], axis=1)
    routed = mm(select_ref[...], back)
    tok_ref[...] = (routed + (own_ref[...].astype(F32) + peer_ref[...].astype(F32))).astype(BF16)

    @pl.when(pl.program_id(0) == 0)
    def _():
        notes = notes_ref[...].astype(F32)
        whole = jnp.sum(notes, axis=0)
        down_ref[...] = jnp.concatenate([whole[0:1] + whole[2:3], whole[1:2] + whole[3:4]], axis=1)
        row = lax.broadcasted_iota(jnp.int32, notes.shape, 1)
        gate_at[...] = jnp.sum(jnp.where((row == 4) | (row == 5), notes, 0.0), axis=1)
        gate = gate_at[...]
        place = place_ref[...]
        at = jnp.zeros(place.shape, F32)
        for r in range(cap):
            at = jnp.where(place == r, gate[:, r : r + 1], at)
        e = lax.broadcasted_iota(jnp.int32, place.shape, 0)
        for k in range(ids_ref.shape[0]):
            mine = jnp.sum(jnp.where(ids_ref[k : k + 1, :] == e, at, 0.0), axis=0, keepdims=True)
            gate_ref[k : k + 1, :] = mine / gates_ref[k : k + 1, :]


def finished(payload, select_t, s_own, s_peer, place, ids_t, gates_t):
    experts, lines, lanes = payload.shape
    tok_rows, half = s_own.shape
    slots = select_t.shape[1]
    cap = slots // experts
    steps = half // (2 * lanes)
    extra = lines - cap * half // lanes
    return pl.pallas_call(
        final_kernel,
        grid=(steps,),
        in_specs=[
            pl.BlockSpec((experts, 2 * cap, lanes), lambda i: (0, i, 0)),
            pl.BlockSpec((experts, extra, lanes), lambda i: (0, lines // extra - 1, 0)),
            pl.BlockSpec((tok_rows, slots), lambda i: (0, 0)),
            pl.BlockSpec((tok_rows, 2 * lanes), lambda i: (0, i)),
            pl.BlockSpec((tok_rows, 2 * lanes), lambda i: (0, i)),
            pl.BlockSpec(place.shape, lambda i: (0, 0)),
            pl.BlockSpec(ids_t.shape, lambda i: (0, 0)),
            pl.BlockSpec(gates_t.shape, lambda i: (0, 0)),
        ],
        out_specs=[
            pl.BlockSpec((tok_rows, 2 * lanes), lambda i: (0, i)),
            pl.BlockSpec(gates_t.shape, lambda i: (0, 0)),
            pl.BlockSpec((1, 2 * lanes), lambda i: (0, 0)),
        ],
        out_shape=[
            jax.ShapeDtypeStruct((tok_rows, half), BF16),
            jax.ShapeDtypeStruct(gates_t.shape, F32),
            jax.ShapeDtypeStruct((1, 2 * lanes), F32),
        ],
        scratch_shapes=[pltpu.VMEM((experts, lanes), F32)],
        name="final",
    )(payload, payload, select_t, s_own, s_peer, place, ids_t, gates_t)


def positions(size):
    return [(i // SIDE**2 % SIDE, i // SIDE % SIDE, i % SIDE) for i in range(size)]


def next_along(x, by):
    pairs = []
    for z, y, x_at in positions(lax.axis_size("ep")):
        here = (z * SIDE + y) * SIDE + x_at
        pairs.append((2 * here, 2 * ((((z + by) % SIDE) * SIDE + y) * SIDE + x_at)))
        pairs.append((2 * here + 1, 2 * ((z * SIDE + (y + by) % SIDE) * SIDE + x_at) + 1))
    return lax.ppermute(x, ("ep", "tp"), pairs)


def plane_groups(size):
    at = positions(size)
    by_z = [[2 * i for i in range(size) if at[i][0] == c] for c in range(SIDE)]
    by_y = [[2 * i + 1 for i in range(size) if at[i][1] == c] for c in range(SIDE)]
    return by_z + by_y


def stage_kernel(a_ref, b_ref, c_ref, d_ref, out_ref):
    pair = a_ref[...].astype(F32) + b_ref[...].astype(F32)
    out_ref[...] = (pair + (c_ref[...].astype(F32) + d_ref[...].astype(F32))).astype(BF16)


def stage_total(pieces):
    rows, cols = pieces[0].shape
    steps = 4
    spec = pl.BlockSpec((rows // steps, cols), lambda i: (i, 0))
    return pl.pallas_call(
        stage_kernel,
        grid=(steps,),
        in_specs=[spec] * len(pieces),
        out_specs=spec,
        out_shape=jax.ShapeDtypeStruct((rows, cols), BF16),
        name="stage_total",
    )(*pieces)


def silu_parts(pre):
    sigmoid = jax.nn.sigmoid(pre)
    return (pre * sigmoid, sigmoid * (1.0 + pre * (1.0 - sigmoid)))


def to_hidden(inputs, cots, w_g, w_u, w_d):
    gate_pre = mm(inputs, w_g)
    up_pre = mm(inputs, w_u)
    active, slope = silu_parts(gate_pre)
    hidden = (active * up_pre).astype(BF16)
    hidden_cot = mm(cots, w_d, COLS)
    gate_part = jnp.sum(hidden.astype(F32) * hidden_cot, axis=1)
    d_gate = (hidden_cot * up_pre * slope).astype(BF16)
    d_up = (hidden_cot * active).astype(BF16)
    return hidden, d_gate, d_up, gate_part


def input_rows(d_both, w_both, first, width):
    return mm(d_both, lax.dynamic_slice_in_dim(w_both, first, width, 0), COLS).astype(BF16)


def layer(tokens, expert_ids, gates, cotangent, w_gate, w_up, w_down, sh_gate, sh_up, sh_down):
    experts = lax.axis_size("ep")
    tok_rows, width = tokens.shape
    top = expert_ids.shape[1]
    cap = 3 * tok_rows * top // (2 * experts)
    slots = experts * cap
    half = width // 2
    tp = lax.axis_index("tp")
    own, other = tp * half, (1 - tp) * half
    w_g, w_u, w_d = w_gate[0], w_up[0], w_down[0]

    ids_t = expert_ids.T
    gates_t = gates.T
    sent, place = routing(tp, ids_t, gates_t, tokens, cotangent, experts, cap)
    got = to_each(sent.reshape(experts, cap, width)).reshape(slots, width)

    s_hidden, s_gate, s_up, _ = to_hidden(tokens, cotangent, sh_gate, sh_up, sh_down)
    hid = s_hidden.shape[1]
    s_both = jnp.concatenate([sh_gate, sh_up], axis=1)
    s_d = jnp.concatenate([s_gate, s_up], axis=1)
    s_other = input_rows(s_d, s_both, other, half)
    s_own = input_rows(s_d, s_both, own, half)
    shared = jnp.concatenate([mm(tokens, s_d, ROWS), mm(cotangent, s_hidden, ROWS)], axis=1).astype(BF16)
    plane = experts // SIDE
    block = width // SIDE**2
    ep = lax.axis_index("ep")
    z, y = lax.div(ep, plane), lax.rem(lax.div(ep, SIDE), SIDE)
    main = jnp.where(tp == 0, z, y)
    step, stride = jnp.where(tp == 0, SIDE, 1), jnp.where(tp == 0, 1, SIDE)
    pieces = []
    for by in range(SIDE):
        first = lax.rem(main + by, SIDE) * step
        pieces.append(
            jnp.concatenate(
                [
                    lax.dynamic_slice_in_dim(shared, (first + j * stride) * block, block, 0)
                    for j in range(SIDE)
                ],
                axis=0,
            )
        )
    arrived = [next_along(pieces[by], by) for by in range(1, SIDE)]
    terms = stage_total(pieces[:1] + arrived).reshape(plane, width // experts, 3 * hid)
    shared_got = lax.all_to_all(
        terms, ("ep", "tp"), 0, 0, tiled=True, axis_index_groups=plane_groups(experts)
    )
    s_peer = swap(s_other)
    w_gu = jnp.concatenate([w_g, w_u], axis=1)
    w_gu_own = lax.dynamic_slice_in_dim(w_gu, own, half, 0)
    w_gu_other = lax.dynamic_slice_in_dim(w_gu, other, half, 0)
    w_d_own = lax.dynamic_slice_in_dim(w_d, own, half, 1)
    w_d_other = lax.dynamic_slice_in_dim(w_d, other, half, 1)

    slot = jnp.arange(slots, dtype=jnp.int32)
    pick = place.T[:, :, None] == (slot[:cap].astype(F32))[None, None, :]
    select_t = pick.astype(BF16).reshape(tok_rows, slots)
    peer = swap(got)
    pre = mm(got[:, :half], w_gu_own) + mm(peer[:, :half], w_gu_other)
    hidden_cot = mm(got[:, half:], w_d_own, COLS) + mm(peer[:, half:], w_d_other, COLS)
    gate_pre, up_pre = pre[:, :hid], pre[:, hid:]
    active, slope = silu_parts(gate_pre)
    hidden = (active * up_pre).astype(BF16)
    gate_part = jnp.sum(hidden.astype(F32) * hidden_cot, axis=1)
    d_both = jnp.concatenate([hidden_cot * up_pre * slope, hidden_cot * active], axis=1).astype(BF16)
    rows_other = mm(d_both, w_gu_other, COLS).astype(BF16)
    rows_own = mm(d_both, w_gu_own, COLS).astype(BF16)
    from_peer = swap(rows_other)
    gate_peer = swap(gate_part)
    extra = 8
    payload = payload_of(rows_own, from_peer, experts, extra)
    gate_sum = jnp.pad((gate_part + gate_peer).reshape(experts, 1, cap), ((0, 0), (0, 0), (0, 128 - cap)))
    high = lax.reduce_precision(gate_sum, 8, 7)
    line = jnp.arange(extra)[None, :, None]
    notes = jnp.where(line == 4, high, jnp.where(line == 5, gate_sum - high, 0.0))
    shared_sum, payload = totals(shared_got, notes, payload)
    back = to_each(payload)
    shared_g, shared_u = shared_sum[:, :hid], shared_sum[:, hid : 2 * hid]
    shared_d = shared_sum[:, 2 * hid :].T

    low = tp == 0
    inputs = jnp.concatenate(
        [jnp.where(low, got[:, :half], peer[:, :half]), jnp.where(low, peer[:, :half], got[:, :half])],
        axis=1,
    )
    cots = jnp.concatenate(
        [jnp.where(low, got[:, half:], peer[:, half:]), jnp.where(low, peer[:, half:], got[:, half:])],
        axis=1,
    )
    grad_g = mm(inputs, d_both[:, :hid], ROWS)
    grad_u = mm(inputs, d_both[:, hid:], ROWS)
    grad_d = mm(hidden, cots, ROWS)

    norms = jnp.concatenate(
        [
            jnp.sum(grad_g * grad_g, axis=1),
            jnp.sum(grad_u * grad_u, axis=1),
            jnp.sum(shared_g * shared_g, axis=1),
            jnp.sum(shared_u * shared_u, axis=1),
        ]
    )
    norms = norms + swap(norms)
    step = width // experts
    gate_norms, up_norms = norms[:width], norms[width : 2 * width]
    shared_gate_norms, shared_up_norms = norms[2 * width : 2 * width + step], norms[2 * width + step :]

    token_grad, gate_grad, down_norms = finished(back, select_t, s_own, s_peer, place, ids_t, gates_t)
    gate_grad = gate_grad.T
    down_norms = down_norms.reshape(hid)
    return (
        token_grad,
        gate_grad,
        grad_g[None],
        grad_u[None],
        grad_d[None],
        shared_g,
        shared_u,
        shared_d,
        gate_norms[None],
        up_norms[None],
        jnp.sum(grad_d * grad_d, axis=1)[None],
        shared_gate_norms,
        shared_up_norms,
        down_norms,
    )


def solution(mesh):
    placed = (
        P("ep", None),
        P("ep", None),
        P("ep", None),
        P("ep", None),
        P("ep", None, "tp"),
        P("ep", None, "tp"),
        P("ep", "tp", None),
        P(None, "tp"),
        P(None, "tp"),
        P("tp", None),
    )
    return jax.shard_map(
        layer,
        mesh=mesh,
        in_specs=placed,
        out_specs=(
            P("ep", "tp"),
            P("ep", None),
            P("ep", None, "tp"),
            P("ep", None, "tp"),
            P("ep", "tp", None),
            P("ep", "tp"),
            P("ep", "tp"),
            P("tp", "ep"),
            P("ep", None),
            P("ep", None),
            P("ep", "tp"),
            P("ep"),
            P("ep"),
            P("tp"),
        ),
        check_vma=False,
    )
```

```python
import jax
import jax.numpy as jnp
from jax import lax
from jax.experimental import pallas as pl
from jax.experimental.pallas import tpu as pltpu
from jax.sharding import PartitionSpec as P


F32 = jnp.float32
BF16 = jnp.bfloat16
ROWS = (((0,), (0,)), ((), ()))
COLS = (((1,), (1,)), ((), ()))
PLAIN = (((1,), (0,)), ((), ()))
SIDE = 4
GRANT = 24 * 1024 * 1024


def mm(a, b, contract=PLAIN):
    return lax.dot_general(a, b, contract, preferred_element_type=F32)


def swap(x):
    return lax.ppermute(x, "tp", [(0, 1), (1, 0)])


def to_each(x):
    return lax.all_to_all(x, "ep", 0, 0, tiled=True)


def routing_kernel(tp_ref, ids_ref, gates_ref, tok_ref, cot_ref, sent_ref, place_ref, place_at, gate_at):
    experts, tok_rows = place_at.shape
    rows, width = sent_ref.shape
    half = width // 2
    steps = pl.num_programs(0)
    block = experts // steps
    cap = rows // block
    step = pl.program_id(0)

    @pl.when(step == 0)
    def _():
        e = lax.broadcasted_iota(jnp.int32, (experts, tok_rows), 0)
        hit = jnp.zeros((experts, tok_rows), F32)
        gate_of = jnp.zeros((experts, tok_rows), F32)
        for k in range(ids_ref.shape[0]):
            name = ids_ref[k : k + 1, :] == e
            hit = jnp.where(name, 1.0, hit)
            gate_of = jnp.where(name, gates_ref[k : k + 1, :], gate_of)
        earlier = lax.broadcasted_iota(jnp.int32, (tok_rows, tok_rows), 0)
        later = lax.broadcasted_iota(jnp.int32, (tok_rows, tok_rows), 1)
        before = jnp.where(earlier < later, 1.0, 0.0).astype(BF16)
        rank = mm(hit.astype(BF16), before)
        place = jnp.where(hit > 0.0, rank, -1.0)
        place_at[...] = place
        gate_at[...] = gate_of
        place_ref[...] = place

    r = lax.broadcasted_iota(jnp.int32, (cap, tok_rows), 0).astype(F32)
    picks, scales = [], []
    for j in range(block):
        at = pl.ds(step * block + j, 1)
        pick = jnp.broadcast_to(place_at[at, :], (cap, tok_rows)) == r
        picks.append(jnp.where(pick, 1.0, 0.0))
        scales.append(jnp.sum(jnp.where(pick, gate_at[at, :], 0.0), axis=1, keepdims=True))
    select = jnp.concatenate(picks, axis=0).astype(BF16)
    scale = jnp.concatenate(scales, axis=0)
    sent_ref[:, :half] = mm(select, tok_ref[...]).astype(BF16)
    sent_ref[:, half:] = (mm(select, cot_ref[...]) * scale).astype(BF16)


def routing(tp, ids_t, gates_t, tokens, cotangent, experts, cap):
    tok_rows, width = tokens.shape
    half = width // 2
    top = ids_t.shape[0]
    steps = 4
    rows = experts * cap // steps
    return pl.pallas_call(
        routing_kernel,
        grid_spec=pltpu.PrefetchScalarGridSpec(
            num_scalar_prefetch=1,
            grid=(steps,),
            in_specs=[
                pl.BlockSpec((top, tok_rows), lambda i, tp: (0, 0)),
                pl.BlockSpec((top, tok_rows), lambda i, tp: (0, 0)),
                pl.BlockSpec((tok_rows, half), lambda i, tp: (0, tp[0])),
                pl.BlockSpec((tok_rows, half), lambda i, tp: (0, tp[0])),
            ],
            out_specs=[
                pl.BlockSpec((rows, width), lambda i, tp: (i, 0)),
                pl.BlockSpec((experts, tok_rows), lambda i, tp: (0, 0)),
            ],
            scratch_shapes=[pltpu.VMEM((experts, tok_rows), F32), pltpu.VMEM((experts, tok_rows), F32)],
        ),
        out_shape=[
            jax.ShapeDtypeStruct((experts * cap, width), BF16),
            jax.ShapeDtypeStruct((experts, tok_rows), F32),
        ],
        name="routing",
    )(tp.reshape(1), ids_t, gates_t, tokens, cotangent)


def payload_kernel(d_ref, w_ref, peer_ref, out_ref):
    block, lines, lanes = out_ref.shape
    cap = peer_ref.shape[0] // block
    own = mm(d_ref[...], w_ref[...], COLS).astype(BF16).astype(F32)
    both = (own + peer_ref[...].astype(F32)).astype(BF16)
    for e in range(block):
        at = slice(e * cap, (e + 1) * cap)
        for c in range(lines // cap):
            out_ref[e, c * cap : (c + 1) * cap, :] = both[at, c * lanes : (c + 1) * lanes]


def payload_of(d_both, w_own, peer, experts, extra):
    slots, half = peer.shape
    steps = 4
    cap = slots // experts
    lines = cap * half // 128
    return pl.pallas_call(
        payload_kernel,
        grid=(steps,),
        in_specs=[
            pl.BlockSpec((slots // steps, d_both.shape[1]), lambda i: (i, 0)),
            pl.BlockSpec(w_own.shape, lambda i: (0, 0)),
            pl.BlockSpec((slots // steps, half), lambda i: (i, 0)),
        ],
        out_specs=pl.BlockSpec((experts // steps, lines, 128), lambda i: (i, 0, 0)),
        out_shape=jax.ShapeDtypeStruct((experts, lines + extra, 128), BF16),
        compiler_params=pltpu.CompilerParams(vmem_limit_bytes=GRANT),
        name="payload",
    )(d_both, w_own, peer)


def total_kernel(got_ref, notes_ref, payload_ref, sums_ref, out_ref, acc):
    step = pl.program_id(0)
    part = jnp.sum(got_ref[...].astype(F32), axis=0)

    @pl.when(step == 0)
    def _():
        acc[...] = part

    @pl.when(step > 0)
    def _():
        acc[...] = acc[...] + part

    @pl.when(step == pl.num_programs(0) - 1)
    def _():
        total = acc[...]
        sums_ref[...] = total
        down = total[:, 2 * (total.shape[1] // 3) :]
        norms = jnp.sum(down * down, axis=0, keepdims=True)
        high = norms.astype(BF16).astype(F32)
        low = norms - high
        lines = out_ref.shape[1:]
        row = lax.broadcasted_iota(jnp.int32, lines, 0)
        marks = jnp.zeros(lines, F32)
        pieces = norms.shape[1] // lines[1]
        for at, value in enumerate((high, low)):
            for c in range(pieces):
                line = value[:, c * lines[1] : (c + 1) * lines[1]]
                marks = jnp.where(row == at * pieces + c, line, marks)
        out_ref[...] = (notes_ref[...] + marks[None]).astype(BF16)


def totals(got, notes, payload):
    size, rows, cols = got.shape
    steps = 2
    experts, extra, lanes = notes.shape
    last = payload.shape[1] // extra - 1
    return pl.pallas_call(
        total_kernel,
        grid=(steps,),
        in_specs=[
            pl.BlockSpec((size // steps, rows, cols), lambda i: (i, 0, 0)),
            pl.BlockSpec((experts, extra, lanes), lambda i: (0, 0, 0)),
            pl.BlockSpec(memory_space=pl.ANY),
        ],
        out_specs=[
            pl.BlockSpec((rows, cols), lambda i: (0, 0)),
            pl.BlockSpec((experts, extra, lanes), lambda i: (0, last, 0)),
        ],
        out_shape=[
            jax.ShapeDtypeStruct((rows, cols), F32),
            jax.ShapeDtypeStruct(payload.shape, BF16),
        ],
        input_output_aliases={2: 1},
        scratch_shapes=[pltpu.VMEM((rows, cols), F32)],
        compiler_params=pltpu.CompilerParams(vmem_limit_bytes=GRANT),
        name="totals",
    )(got, notes, payload)


def final_kernel(rows_ref, notes_ref, select_ref, own_ref, peer_ref, place_ref, ids_ref, gates_ref, tok_ref, gate_ref, down_ref, gate_at):
    experts, lines, lanes = rows_ref.shape
    tiles = own_ref.shape[1] // lanes
    cap = lines // tiles
    columns = [rows_ref[:, c * cap : (c + 1) * cap, :].reshape(experts * cap, lanes) for c in range(tiles)]
    back = jnp.concatenate(columns, axis=1)
    routed = mm(select_ref[...], back)
    tok_ref[...] = (routed + (own_ref[...].astype(F32) + peer_ref[...].astype(F32))).astype(BF16)

    @pl.when(pl.program_id(0) == 0)
    def _():
        notes = notes_ref[...].astype(F32)
        whole = jnp.sum(notes, axis=0)
        down_ref[...] = jnp.concatenate([whole[0:1] + whole[2:3], whole[1:2] + whole[3:4]], axis=1)
        row = lax.broadcasted_iota(jnp.int32, notes.shape, 1)
        gate_at[...] = jnp.sum(jnp.where((row == 4) | (row == 5), notes, 0.0), axis=1)
        gate = gate_at[...]
        place = place_ref[...]
        at = jnp.zeros(place.shape, F32)
        for r in range(cap):
            at = jnp.where(place == r, gate[:, r : r + 1], at)
        e = lax.broadcasted_iota(jnp.int32, place.shape, 0)
        for k in range(ids_ref.shape[0]):
            mine = jnp.sum(jnp.where(ids_ref[k : k + 1, :] == e, at, 0.0), axis=0, keepdims=True)
            gate_ref[k : k + 1, :] = mine / gates_ref[k : k + 1, :]


def finished(payload, select_t, s_own, s_peer, place, ids_t, gates_t):
    experts, lines, lanes = payload.shape
    tok_rows, half = s_own.shape
    slots = select_t.shape[1]
    cap = slots // experts
    steps = 2
    cols = half // steps
    tiles = cols // lanes
    extra = lines - cap * half // lanes
    return pl.pallas_call(
        final_kernel,
        grid=(steps,),
        in_specs=[
            pl.BlockSpec((experts, tiles * cap, lanes), lambda i: (0, i, 0)),
            pl.BlockSpec((experts, extra, lanes), lambda i: (0, lines // extra - 1, 0)),
            pl.BlockSpec((tok_rows, slots), lambda i: (0, 0)),
            pl.BlockSpec((tok_rows, cols), lambda i: (0, i)),
            pl.BlockSpec((tok_rows, cols), lambda i: (0, i)),
            pl.BlockSpec(place.shape, lambda i: (0, 0)),
            pl.BlockSpec(ids_t.shape, lambda i: (0, 0)),
            pl.BlockSpec(gates_t.shape, lambda i: (0, 0)),
        ],
        out_specs=[
            pl.BlockSpec((tok_rows, cols), lambda i: (0, i)),
            pl.BlockSpec(gates_t.shape, lambda i: (0, 0)),
            pl.BlockSpec((1, 2 * lanes), lambda i: (0, 0)),
        ],
        out_shape=[
            jax.ShapeDtypeStruct((tok_rows, half), BF16),
            jax.ShapeDtypeStruct(gates_t.shape, F32),
            jax.ShapeDtypeStruct((1, 2 * lanes), F32),
        ],
        scratch_shapes=[pltpu.VMEM((experts, lanes), F32)],
        compiler_params=pltpu.CompilerParams(vmem_limit_bytes=GRANT),
        name="final",
    )(payload, payload, select_t, s_own, s_peer, place, ids_t, gates_t)


def positions(size):
    return [(i // SIDE**2 % SIDE, i // SIDE % SIDE, i % SIDE) for i in range(size)]


def next_along(x, by):
    pairs = []
    for z, y, x_at in positions(lax.axis_size("ep")):
        here = (z * SIDE + y) * SIDE + x_at
        pairs.append((2 * here, 2 * ((((z + by) % SIDE) * SIDE + y) * SIDE + x_at)))
        pairs.append((2 * here + 1, 2 * ((z * SIDE + (y + by) % SIDE) * SIDE + x_at) + 1))
    return lax.ppermute(x, ("ep", "tp"), pairs)


def plane_groups(size):
    at = positions(size)
    by_z = [[2 * i for i in range(size) if at[i][0] == c] for c in range(SIDE)]
    by_y = [[2 * i + 1 for i in range(size) if at[i][1] == c] for c in range(SIDE)]
    return by_z + by_y


def stage_kernel(a_ref, b_ref, c_ref, d_ref, out_ref):
    pair = a_ref[...].astype(F32) + b_ref[...].astype(F32)
    out_ref[...] = (pair + (c_ref[...].astype(F32) + d_ref[...].astype(F32))).astype(BF16)


def stage_total(pieces):
    rows, cols = pieces[0].shape
    steps = 2
    spec = pl.BlockSpec((rows // steps, cols), lambda i: (i, 0))
    return pl.pallas_call(
        stage_kernel,
        grid=(steps,),
        in_specs=[spec] * len(pieces),
        out_specs=spec,
        out_shape=jax.ShapeDtypeStruct((rows, cols), BF16),
        compiler_params=pltpu.CompilerParams(vmem_limit_bytes=GRANT),
        name="stage_total",
    )(*pieces)


def silu_parts(pre):
    sigmoid = jax.nn.sigmoid(pre)
    return (pre * sigmoid, sigmoid * (1.0 + pre * (1.0 - sigmoid)))


def to_hidden(inputs, cots, w_g, w_u, w_d):
    gate_pre = mm(inputs, w_g)
    up_pre = mm(inputs, w_u)
    active, slope = silu_parts(gate_pre)
    hidden = (active * up_pre).astype(BF16)
    hidden_cot = mm(cots, w_d, COLS)
    gate_part = jnp.sum(hidden.astype(F32) * hidden_cot, axis=1)
    d_gate = (hidden_cot * up_pre * slope).astype(BF16)
    d_up = (hidden_cot * active).astype(BF16)
    return hidden, d_gate, d_up, gate_part


def input_rows(d_both, w_both, first, width):
    return mm(d_both, lax.dynamic_slice_in_dim(w_both, first, width, 0), COLS).astype(BF16)


def layer(tokens, expert_ids, gates, cotangent, w_gate, w_up, w_down, sh_gate, sh_up, sh_down):
    experts = lax.axis_size("ep")
    tok_rows, width = tokens.shape
    top = expert_ids.shape[1]
    cap = 3 * tok_rows * top // (2 * experts)
    slots = experts * cap
    half = width // 2
    tp = lax.axis_index("tp")
    own, other = tp * half, (1 - tp) * half
    w_g, w_u, w_d = w_gate[0], w_up[0], w_down[0]

    ids_t = expert_ids.T
    gates_t = gates.T
    sent, place = routing(tp, ids_t, gates_t, tokens, cotangent, experts, cap)
    got = to_each(sent.reshape(experts, cap, width)).reshape(slots, width)

    s_hidden, s_gate, s_up, _ = to_hidden(tokens, cotangent, sh_gate, sh_up, sh_down)
    hid = s_hidden.shape[1]
    s_both = jnp.concatenate([sh_gate, sh_up], axis=1)
    s_d = jnp.concatenate([s_gate, s_up], axis=1)
    s_other = input_rows(s_d, s_both, other, half)
    s_own = input_rows(s_d, s_both, own, half)
    shared = jnp.concatenate([mm(tokens, s_d, ROWS), mm(cotangent, s_hidden, ROWS)], axis=1).astype(BF16)
    plane = experts // SIDE
    block = width // SIDE**2
    ep = lax.axis_index("ep")
    z, y = lax.div(ep, plane), lax.rem(lax.div(ep, SIDE), SIDE)
    main = jnp.where(tp == 0, z, y)
    step, stride = jnp.where(tp == 0, SIDE, 1), jnp.where(tp == 0, 1, SIDE)
    pieces = []
    for by in range(SIDE):
        first = lax.rem(main + by, SIDE) * step
        pieces.append(
            jnp.concatenate(
                [
                    lax.dynamic_slice_in_dim(shared, (first + j * stride) * block, block, 0)
                    for j in range(SIDE)
                ],
                axis=0,
            )
        )
    arrived = [next_along(pieces[by], by) for by in range(1, SIDE)]
    terms = stage_total(pieces[:1] + arrived).reshape(plane, width // experts, 3 * hid)
    shared_got = lax.all_to_all(
        terms, ("ep", "tp"), 0, 0, tiled=True, axis_index_groups=plane_groups(experts)
    )
    s_peer = swap(s_other)
    w_gu = jnp.concatenate([w_g, w_u], axis=1)
    w_gu_own = lax.dynamic_slice_in_dim(w_gu, own, half, 0)
    w_gu_other = lax.dynamic_slice_in_dim(w_gu, other, half, 0)
    w_d_own = lax.dynamic_slice_in_dim(w_d, own, half, 1)
    w_d_other = lax.dynamic_slice_in_dim(w_d, other, half, 1)

    slot = jnp.arange(slots, dtype=jnp.int32)
    pick = place.T[:, :, None] == (slot[:cap].astype(F32))[None, None, :]
    select_t = pick.astype(BF16).reshape(tok_rows, slots)
    peer = swap(got)
    pre = mm(got[:, :half], w_gu_own) + mm(peer[:, :half], w_gu_other)
    hidden_cot = mm(got[:, half:], w_d_own, COLS) + mm(peer[:, half:], w_d_other, COLS)
    gate_pre, up_pre = pre[:, :hid], pre[:, hid:]
    active, slope = silu_parts(gate_pre)
    hidden = (active * up_pre).astype(BF16)
    gate_part = jnp.sum(hidden.astype(F32) * hidden_cot, axis=1)
    d_both = jnp.concatenate([hidden_cot * up_pre * slope, hidden_cot * active], axis=1).astype(BF16)
    rows_other = mm(d_both, w_gu_other, COLS).astype(BF16)
    from_peer = swap(rows_other)
    gate_peer = swap(gate_part)
    extra = 8
    payload = payload_of(d_both, w_gu_own, from_peer, experts, extra)
    gate_sum = jnp.pad((gate_part + gate_peer).reshape(experts, 1, cap), ((0, 0), (0, 0), (0, 128 - cap)))
    high = lax.reduce_precision(gate_sum, 8, 7)
    line = jnp.arange(extra)[None, :, None]
    notes = jnp.where(line == 4, high, jnp.where(line == 5, gate_sum - high, 0.0))
    shared_sum, payload = totals(shared_got, notes, payload)
    back = to_each(payload)
    shared_g, shared_u = shared_sum[:, :hid], shared_sum[:, hid : 2 * hid]
    shared_d = shared_sum[:, 2 * hid :].T

    low = tp == 0
    inputs = jnp.concatenate(
        [jnp.where(low, got[:, :half], peer[:, :half]), jnp.where(low, peer[:, :half], got[:, :half])],
        axis=1,
    )
    cots = jnp.concatenate(
        [jnp.where(low, got[:, half:], peer[:, half:]), jnp.where(low, peer[:, half:], got[:, half:])],
        axis=1,
    )
    grad_g = mm(inputs, d_both[:, :hid], ROWS)
    grad_u = mm(inputs, d_both[:, hid:], ROWS)
    grad_d = mm(hidden, cots, ROWS)

    norms = jnp.concatenate(
        [
            jnp.sum(grad_g * grad_g, axis=1),
            jnp.sum(grad_u * grad_u, axis=1),
            jnp.sum(shared_g * shared_g, axis=1),
            jnp.sum(shared_u * shared_u, axis=1),
        ]
    )
    norms = norms + swap(norms)
    step = width // experts
    gate_norms, up_norms = norms[:width], norms[width : 2 * width]
    shared_gate_norms, shared_up_norms = norms[2 * width : 2 * width + step], norms[2 * width + step :]

    token_grad, gate_grad, down_norms = finished(back, select_t, s_own, s_peer, place, ids_t, gates_t)
    gate_grad = gate_grad.T
    down_norms = down_norms.reshape(hid)
    return (
        token_grad,
        gate_grad,
        grad_g[None],
        grad_u[None],
        grad_d[None],
        shared_g,
        shared_u,
        shared_d,
        gate_norms[None],
        up_norms[None],
        jnp.sum(grad_d * grad_d, axis=1)[None],
        shared_gate_norms,
        shared_up_norms,
        down_norms,
    )


def solution(mesh):
    placed = (
        P("ep", None),
        P("ep", None),
        P("ep", None),
        P("ep", None),
        P("ep", None, "tp"),
        P("ep", None, "tp"),
        P("ep", "tp", None),
        P(None, "tp"),
        P(None, "tp"),
        P("tp", None),
    )
    return jax.shard_map(
        layer,
        mesh=mesh,
        in_specs=placed,
        out_specs=(
            P("ep", "tp"),
            P("ep", None),
            P("ep", None, "tp"),
            P("ep", None, "tp"),
            P("ep", "tp", None),
            P("ep", "tp"),
            P("ep", "tp"),
            P("tp", "ep"),
            P("ep", None),
            P("ep", None),
            P("ep", "tp"),
            P("ep"),
            P("ep"),
            P("tp"),
        ),
        check_vma=False,
    )
```

```python
import jax
import jax.numpy as jnp
from jax import lax
from jax.experimental import pallas as pl
from jax.experimental.pallas import tpu as pltpu
from jax.sharding import PartitionSpec as P


F32 = jnp.float32
BF16 = jnp.bfloat16
ROWS = (((0,), (0,)), ((), ()))
COLS = (((1,), (1,)), ((), ()))
PLAIN = (((1,), (0,)), ((), ()))
SIDE = 4
TURN = 53
GRANT = 24 * 1024 * 1024


def mm(a, b, contract=PLAIN):
    return lax.dot_general(a, b, contract, preferred_element_type=F32)


def swap(x):
    return lax.ppermute(x, "tp", [(0, 1), (1, 0)])


def turn_of(e, size):
    return (TURN * e) & (size - 1)


def to_each(x):
    size = x.shape[0]
    order = sorted(range(size), key=lambda e: turn_of(e, size))
    return lax.all_to_all(x, "ep", 0, 0, tiled=True, axis_index_groups=[order])


def routing_kernel(tp_ref, ids_ref, gates_ref, tok_ref, cot_ref, sent_ref, place_ref, place_at, gate_at):
    experts, tok_rows = place_at.shape
    rows, width = sent_ref.shape
    half = width // 2
    steps = pl.num_programs(0)
    block = experts // steps
    cap = rows // block
    step = pl.program_id(0)

    @pl.when(step == 0)
    def _():
        e = lax.broadcasted_iota(jnp.int32, (experts, tok_rows), 0)
        hit = jnp.zeros((experts, tok_rows), F32)
        gate_of = jnp.zeros((experts, tok_rows), F32)
        for k in range(ids_ref.shape[0]):
            name = turn_of(ids_ref[k : k + 1, :], experts) == e
            hit = jnp.where(name, 1.0, hit)
            gate_of = jnp.where(name, gates_ref[k : k + 1, :], gate_of)
        earlier = lax.broadcasted_iota(jnp.int32, (tok_rows, tok_rows), 0)
        later = lax.broadcasted_iota(jnp.int32, (tok_rows, tok_rows), 1)
        before = jnp.where(earlier < later, 1.0, 0.0).astype(BF16)
        rank = mm(hit.astype(BF16), before)
        place = jnp.where(hit > 0.0, rank, -1.0)
        place_at[...] = place
        gate_at[...] = gate_of
        place_ref[...] = place

    r = lax.broadcasted_iota(jnp.int32, (cap, tok_rows), 0).astype(F32)
    picks, scales = [], []
    for j in range(block):
        at = pl.ds(step * block + j, 1)
        pick = jnp.broadcast_to(place_at[at, :], (cap, tok_rows)) == r
        picks.append(jnp.where(pick, 1.0, 0.0))
        scales.append(jnp.sum(jnp.where(pick, gate_at[at, :], 0.0), axis=1, keepdims=True))
    select = jnp.concatenate(picks, axis=0).astype(BF16)
    scale = jnp.concatenate(scales, axis=0)
    sent_ref[:, :half] = mm(select, tok_ref[...]).astype(BF16)
    sent_ref[:, half:] = (mm(select, cot_ref[...]) * scale).astype(BF16)


def routing(tp, ids_t, gates_t, tokens, cotangent, experts, cap):
    tok_rows, width = tokens.shape
    half = width // 2
    top = ids_t.shape[0]
    steps = 4
    rows = experts * cap // steps
    return pl.pallas_call(
        routing_kernel,
        grid_spec=pltpu.PrefetchScalarGridSpec(
            num_scalar_prefetch=1,
            grid=(steps,),
            in_specs=[
                pl.BlockSpec((top, tok_rows), lambda i, tp: (0, 0)),
                pl.BlockSpec((top, tok_rows), lambda i, tp: (0, 0)),
                pl.BlockSpec((tok_rows, half), lambda i, tp: (0, tp[0])),
                pl.BlockSpec((tok_rows, half), lambda i, tp: (0, tp[0])),
            ],
            out_specs=[
                pl.BlockSpec((rows, width), lambda i, tp: (i, 0)),
                pl.BlockSpec((experts, tok_rows), lambda i, tp: (0, 0)),
            ],
            scratch_shapes=[pltpu.VMEM((experts, tok_rows), F32), pltpu.VMEM((experts, tok_rows), F32)],
        ),
        out_shape=[
            jax.ShapeDtypeStruct((experts * cap, width), BF16),
            jax.ShapeDtypeStruct((experts, tok_rows), F32),
        ],
        name="routing",
    )(tp.reshape(1), ids_t, gates_t, tokens, cotangent)


def payload_kernel(d_ref, w_ref, peer_ref, out_ref):
    block, lines, lanes = out_ref.shape
    cap = peer_ref.shape[0] // block
    own = mm(d_ref[...], w_ref[...], COLS).astype(BF16).astype(F32)
    both = (own + peer_ref[...].astype(F32)).astype(BF16)
    for e in range(block):
        at = slice(e * cap, (e + 1) * cap)
        for c in range(lines // cap):
            out_ref[e, c * cap : (c + 1) * cap, :] = both[at, c * lanes : (c + 1) * lanes]


def payload_of(d_both, w_own, peer, experts, extra):
    slots, half = peer.shape
    steps = 4
    cap = slots // experts
    lines = cap * half // 128
    return pl.pallas_call(
        payload_kernel,
        grid=(steps,),
        in_specs=[
            pl.BlockSpec((slots // steps, d_both.shape[1]), lambda i: (i, 0)),
            pl.BlockSpec(w_own.shape, lambda i: (0, 0)),
            pl.BlockSpec((slots // steps, half), lambda i: (i, 0)),
        ],
        out_specs=pl.BlockSpec((experts // steps, lines, 128), lambda i: (i, 0, 0)),
        out_shape=jax.ShapeDtypeStruct((experts, lines + extra, 128), BF16),
        compiler_params=pltpu.CompilerParams(vmem_limit_bytes=GRANT),
        name="payload",
    )(d_both, w_own, peer)


def total_kernel(got_ref, notes_ref, payload_ref, sums_ref, out_ref, acc):
    step = pl.program_id(0)
    part = jnp.sum(got_ref[...].astype(F32), axis=0)

    @pl.when(step == 0)
    def _():
        acc[...] = part

    @pl.when(step > 0)
    def _():
        acc[...] = acc[...] + part

    @pl.when(step == pl.num_programs(0) - 1)
    def _():
        total = acc[...]
        sums_ref[...] = total
        down = total[:, 2 * (total.shape[1] // 3) :]
        norms = jnp.sum(down * down, axis=0, keepdims=True)
        high = norms.astype(BF16).astype(F32)
        low = norms - high
        lines = out_ref.shape[1:]
        row = lax.broadcasted_iota(jnp.int32, lines, 0)
        marks = jnp.zeros(lines, F32)
        pieces = norms.shape[1] // lines[1]
        for at, value in enumerate((high, low)):
            for c in range(pieces):
                line = value[:, c * lines[1] : (c + 1) * lines[1]]
                marks = jnp.where(row == at * pieces + c, line, marks)
        out_ref[...] = (notes_ref[...] + marks[None]).astype(BF16)


def totals(got, notes, payload):
    size, rows, cols = got.shape
    steps = 2
    experts, extra, lanes = notes.shape
    last = payload.shape[1] // extra - 1
    return pl.pallas_call(
        total_kernel,
        grid=(steps,),
        in_specs=[
            pl.BlockSpec((size // steps, rows, cols), lambda i: (i, 0, 0)),
            pl.BlockSpec((experts, extra, lanes), lambda i: (0, 0, 0)),
            pl.BlockSpec(memory_space=pl.ANY),
        ],
        out_specs=[
            pl.BlockSpec((rows, cols), lambda i: (0, 0)),
            pl.BlockSpec((experts, extra, lanes), lambda i: (0, last, 0)),
        ],
        out_shape=[
            jax.ShapeDtypeStruct((rows, cols), F32),
            jax.ShapeDtypeStruct(payload.shape, BF16),
        ],
        input_output_aliases={2: 1},
        scratch_shapes=[pltpu.VMEM((rows, cols), F32)],
        compiler_params=pltpu.CompilerParams(vmem_limit_bytes=GRANT),
        name="totals",
    )(got, notes, payload)


def final_kernel(rows_ref, notes_ref, select_ref, own_ref, peer_ref, place_ref, ids_ref, gates_ref, tok_ref, gate_ref, down_ref, gate_at):
    experts, lines, lanes = rows_ref.shape
    tiles = own_ref.shape[1] // lanes
    cap = lines // tiles
    columns = [rows_ref[:, c * cap : (c + 1) * cap, :].reshape(experts * cap, lanes) for c in range(tiles)]
    back = jnp.concatenate(columns, axis=1)
    routed = mm(select_ref[...], back)
    tok_ref[...] = (routed + (own_ref[...].astype(F32) + peer_ref[...].astype(F32))).astype(BF16)

    @pl.when(pl.program_id(0) == 0)
    def _():
        notes = notes_ref[...].astype(F32)
        whole = jnp.sum(notes, axis=0)
        down_ref[...] = jnp.concatenate([whole[0:1] + whole[2:3], whole[1:2] + whole[3:4]], axis=1)
        row = lax.broadcasted_iota(jnp.int32, notes.shape, 1)
        gate_at[...] = jnp.sum(jnp.where((row == 4) | (row == 5), notes, 0.0), axis=1)
        gate = gate_at[...]
        place = place_ref[...]
        at = jnp.zeros(place.shape, F32)
        for r in range(cap):
            at = jnp.where(place == r, gate[:, r : r + 1], at)
        e = lax.broadcasted_iota(jnp.int32, place.shape, 0)
        for k in range(ids_ref.shape[0]):
            mine = jnp.sum(jnp.where(turn_of(ids_ref[k : k + 1, :], experts) == e, at, 0.0), axis=0, keepdims=True)
            gate_ref[k : k + 1, :] = mine / gates_ref[k : k + 1, :]


def finished(payload, select_t, s_own, s_peer, place, ids_t, gates_t):
    experts, lines, lanes = payload.shape
    tok_rows, half = s_own.shape
    slots = select_t.shape[1]
    cap = slots // experts
    steps = 2
    cols = half // steps
    tiles = cols // lanes
    extra = lines - cap * half // lanes
    return pl.pallas_call(
        final_kernel,
        grid=(steps,),
        in_specs=[
            pl.BlockSpec((experts, tiles * cap, lanes), lambda i: (0, i, 0)),
            pl.BlockSpec((experts, extra, lanes), lambda i: (0, lines // extra - 1, 0)),
            pl.BlockSpec((tok_rows, slots), lambda i: (0, 0)),
            pl.BlockSpec((tok_rows, cols), lambda i: (0, i)),
            pl.BlockSpec((tok_rows, cols), lambda i: (0, i)),
            pl.BlockSpec(place.shape, lambda i: (0, 0)),
            pl.BlockSpec(ids_t.shape, lambda i: (0, 0)),
            pl.BlockSpec(gates_t.shape, lambda i: (0, 0)),
        ],
        out_specs=[
            pl.BlockSpec((tok_rows, cols), lambda i: (0, i)),
            pl.BlockSpec(gates_t.shape, lambda i: (0, 0)),
            pl.BlockSpec((1, 2 * lanes), lambda i: (0, 0)),
        ],
        out_shape=[
            jax.ShapeDtypeStruct((tok_rows, half), BF16),
            jax.ShapeDtypeStruct(gates_t.shape, F32),
            jax.ShapeDtypeStruct((1, 2 * lanes), F32),
        ],
        scratch_shapes=[pltpu.VMEM((experts, lanes), F32)],
        compiler_params=pltpu.CompilerParams(vmem_limit_bytes=GRANT),
        name="final",
    )(payload, payload, select_t, s_own, s_peer, place, ids_t, gates_t)


def positions(size):
    return [(i // SIDE**2 % SIDE, i // SIDE % SIDE, i % SIDE) for i in range(size)]


def next_along(x, by):
    pairs = []
    for z, y, x_at in positions(lax.axis_size("ep")):
        here = (z * SIDE + y) * SIDE + x_at
        pairs.append((2 * here, 2 * ((((z + by) % SIDE) * SIDE + y) * SIDE + x_at)))
        pairs.append((2 * here + 1, 2 * ((z * SIDE + (y + by) % SIDE) * SIDE + x_at) + 1))
    return lax.ppermute(x, ("ep", "tp"), pairs)


def plane_groups(size):
    at = positions(size)
    by_z = [[2 * i for i in range(size) if at[i][0] == c] for c in range(SIDE)]
    by_y = [[2 * i + 1 for i in range(size) if at[i][1] == c] for c in range(SIDE)]
    return by_z + by_y


def stage_kernel(a_ref, b_ref, c_ref, d_ref, out_ref):
    pair = a_ref[...].astype(F32) + b_ref[...].astype(F32)
    out_ref[...] = (pair + (c_ref[...].astype(F32) + d_ref[...].astype(F32))).astype(BF16)


def stage_total(pieces):
    rows, cols = pieces[0].shape
    steps = 2
    spec = pl.BlockSpec((rows // steps, cols), lambda i: (i, 0))
    return pl.pallas_call(
        stage_kernel,
        grid=(steps,),
        in_specs=[spec] * len(pieces),
        out_specs=spec,
        out_shape=jax.ShapeDtypeStruct((rows, cols), BF16),
        compiler_params=pltpu.CompilerParams(vmem_limit_bytes=GRANT),
        name="stage_total",
    )(*pieces)


def silu_parts(pre):
    sigmoid = jax.nn.sigmoid(pre)
    return (pre * sigmoid, sigmoid * (1.0 + pre * (1.0 - sigmoid)))


def to_hidden(inputs, cots, w_g, w_u, w_d):
    gate_pre = mm(inputs, w_g)
    up_pre = mm(inputs, w_u)
    active, slope = silu_parts(gate_pre)
    hidden = (active * up_pre).astype(BF16)
    hidden_cot = mm(cots, w_d, COLS)
    gate_part = jnp.sum(hidden.astype(F32) * hidden_cot, axis=1)
    d_gate = (hidden_cot * up_pre * slope).astype(BF16)
    d_up = (hidden_cot * active).astype(BF16)
    return hidden, d_gate, d_up, gate_part


def input_rows(d_both, w_both, first, width):
    return mm(d_both, lax.dynamic_slice_in_dim(w_both, first, width, 0), COLS).astype(BF16)


def layer(tokens, expert_ids, gates, cotangent, w_gate, w_up, w_down, sh_gate, sh_up, sh_down):
    experts = lax.axis_size("ep")
    tok_rows, width = tokens.shape
    top = expert_ids.shape[1]
    cap = 3 * tok_rows * top // (2 * experts)
    slots = experts * cap
    half = width // 2
    tp = lax.axis_index("tp")
    own, other = tp * half, (1 - tp) * half
    w_g, w_u, w_d = w_gate[0], w_up[0], w_down[0]

    ids_t = expert_ids.T
    gates_t = gates.T
    sent, place = routing(tp, ids_t, gates_t, tokens, cotangent, experts, cap)
    got = to_each(sent.reshape(experts, cap, width)).reshape(slots, width)

    s_hidden, s_gate, s_up, _ = to_hidden(tokens, cotangent, sh_gate, sh_up, sh_down)
    hid = s_hidden.shape[1]
    s_both = jnp.concatenate([sh_gate, sh_up], axis=1)
    s_d = jnp.concatenate([s_gate, s_up], axis=1)
    s_other = input_rows(s_d, s_both, other, half)
    s_own = input_rows(s_d, s_both, own, half)
    shared = jnp.concatenate([mm(tokens, s_d, ROWS), mm(cotangent, s_hidden, ROWS)], axis=1).astype(BF16)
    plane = experts // SIDE
    block = width // SIDE**2
    ep = lax.axis_index("ep")
    z, y = lax.div(ep, plane), lax.rem(lax.div(ep, SIDE), SIDE)
    main = jnp.where(tp == 0, z, y)
    step, stride = jnp.where(tp == 0, SIDE, 1), jnp.where(tp == 0, 1, SIDE)
    pieces = []
    for by in range(SIDE):
        first = lax.rem(main + by, SIDE) * step
        pieces.append(
            jnp.concatenate(
                [
                    lax.dynamic_slice_in_dim(shared, (first + j * stride) * block, block, 0)
                    for j in range(SIDE)
                ],
                axis=0,
            )
        )
    arrived = [next_along(pieces[by], by) for by in range(1, SIDE)]
    terms = stage_total(pieces[:1] + arrived).reshape(plane, width // experts, 3 * hid)
    shared_got = lax.all_to_all(
        terms, ("ep", "tp"), 0, 0, tiled=True, axis_index_groups=plane_groups(experts)
    )
    s_peer = swap(s_other)
    w_gu = jnp.concatenate([w_g, w_u], axis=1)
    w_gu_own = lax.dynamic_slice_in_dim(w_gu, own, half, 0)
    w_gu_other = lax.dynamic_slice_in_dim(w_gu, other, half, 0)
    w_d_own = lax.dynamic_slice_in_dim(w_d, own, half, 1)
    w_d_other = lax.dynamic_slice_in_dim(w_d, other, half, 1)

    slot = jnp.arange(slots, dtype=jnp.int32)
    pick = place.T[:, :, None] == (slot[:cap].astype(F32))[None, None, :]
    select_t = pick.astype(BF16).reshape(tok_rows, slots)
    peer = swap(got)
    pre = mm(got[:, :half], w_gu_own) + mm(peer[:, :half], w_gu_other)
    hidden_cot = mm(got[:, half:], w_d_own, COLS) + mm(peer[:, half:], w_d_other, COLS)
    gate_pre, up_pre = pre[:, :hid], pre[:, hid:]
    active, slope = silu_parts(gate_pre)
    hidden = (active * up_pre).astype(BF16)
    gate_part = jnp.sum(hidden.astype(F32) * hidden_cot, axis=1)
    d_both = jnp.concatenate([hidden_cot * up_pre * slope, hidden_cot * active], axis=1).astype(BF16)
    rows_other = mm(d_both, w_gu_other, COLS).astype(BF16)
    from_peer = swap(rows_other)
    gate_peer = swap(gate_part)
    extra = 8
    payload = payload_of(d_both, w_gu_own, from_peer, experts, extra)
    gate_sum = jnp.pad((gate_part + gate_peer).reshape(experts, 1, cap), ((0, 0), (0, 0), (0, 128 - cap)))
    high = lax.reduce_precision(gate_sum, 8, 7)
    line = jnp.arange(extra)[None, :, None]
    notes = jnp.where(line == 4, high, jnp.where(line == 5, gate_sum - high, 0.0))
    shared_sum, payload = totals(shared_got, notes, payload)
    back = to_each(payload)
    shared_g, shared_u = shared_sum[:, :hid], shared_sum[:, hid : 2 * hid]
    shared_d = shared_sum[:, 2 * hid :].T

    low = tp == 0
    inputs = jnp.concatenate(
        [jnp.where(low, got[:, :half], peer[:, :half]), jnp.where(low, peer[:, :half], got[:, :half])],
        axis=1,
    )
    cots = jnp.concatenate(
        [jnp.where(low, got[:, half:], peer[:, half:]), jnp.where(low, peer[:, half:], got[:, half:])],
        axis=1,
    )
    grad_g = mm(inputs, d_both[:, :hid], ROWS)
    grad_u = mm(inputs, d_both[:, hid:], ROWS)
    grad_d = mm(hidden, cots, ROWS)

    norms = jnp.concatenate(
        [
            jnp.sum(grad_g * grad_g, axis=1),
            jnp.sum(grad_u * grad_u, axis=1),
            jnp.sum(shared_g * shared_g, axis=1),
            jnp.sum(shared_u * shared_u, axis=1),
        ]
    )
    norms = norms + swap(norms)
    step = width // experts
    gate_norms, up_norms = norms[:width], norms[width : 2 * width]
    shared_gate_norms, shared_up_norms = norms[2 * width : 2 * width + step], norms[2 * width + step :]

    token_grad, gate_grad, down_norms = finished(back, select_t, s_own, s_peer, place, ids_t, gates_t)
    gate_grad = gate_grad.T
    down_norms = down_norms.reshape(hid)
    return (
        token_grad,
        gate_grad,
        grad_g[None],
        grad_u[None],
        grad_d[None],
        shared_g,
        shared_u,
        shared_d,
        gate_norms[None],
        up_norms[None],
        jnp.sum(grad_d * grad_d, axis=1)[None],
        shared_gate_norms,
        shared_up_norms,
        down_norms,
    )


def solution(mesh):
    placed = (
        P("ep", None),
        P("ep", None),
        P("ep", None),
        P("ep", None),
        P("ep", None, "tp"),
        P("ep", None, "tp"),
        P("ep", "tp", None),
        P(None, "tp"),
        P(None, "tp"),
        P("tp", None),
    )
    return jax.shard_map(
        layer,
        mesh=mesh,
        in_specs=placed,
        out_specs=(
            P("ep", "tp"),
            P("ep", None),
            P("ep", None, "tp"),
            P("ep", None, "tp"),
            P("ep", "tp", None),
            P("ep", "tp"),
            P("ep", "tp"),
            P("tp", "ep"),
            P("ep", None),
            P("ep", None),
            P("ep", "tp"),
            P("ep"),
            P("ep"),
            P("tp"),
        ),
        check_vma=False,
    )
```

```python
import jax
import jax.numpy as jnp
from jax import lax
from jax.experimental import pallas as pl
from jax.experimental.pallas import tpu as pltpu
from jax.sharding import PartitionSpec as P


F32 = jnp.float32
BF16 = jnp.bfloat16
ROWS = (((0,), (0,)), ((), ()))
COLS = (((1,), (1,)), ((), ()))
PLAIN = (((1,), (0,)), ((), ()))
SIDE = 4
TURN = 53
GRANT = 24 * 1024 * 1024


def mm(a, b, contract=PLAIN):
    return lax.dot_general(a, b, contract, preferred_element_type=F32)


def swap(x):
    return lax.ppermute(x, "tp", [(0, 1), (1, 0)])


def turn_of(e, size):
    return (TURN * e) & (size - 1)


def to_each(x):
    size = x.shape[0]
    order = sorted(range(size), key=lambda e: turn_of(e, size))
    return lax.all_to_all(x, "ep", 0, 0, tiled=True, axis_index_groups=[order])


def routing_kernel(tp_ref, ids_ref, gates_ref, tok_ref, cot_ref, sent_ref, place_ref, place_at, gate_at):
    experts, tok_rows = place_at.shape
    rows, width = sent_ref.shape
    half = width // 2
    steps = pl.num_programs(0)
    block = experts // steps
    cap = rows // block
    step = pl.program_id(0)

    @pl.when(step == 0)
    def _():
        e = lax.broadcasted_iota(jnp.int32, (experts, tok_rows), 0)
        hit = jnp.zeros((experts, tok_rows), F32)
        gate_of = jnp.zeros((experts, tok_rows), F32)
        for k in range(ids_ref.shape[0]):
            name = turn_of(ids_ref[k : k + 1, :], experts) == e
            hit = jnp.where(name, 1.0, hit)
            gate_of = jnp.where(name, gates_ref[k : k + 1, :], gate_of)
        earlier = lax.broadcasted_iota(jnp.int32, (tok_rows, tok_rows), 0)
        later = lax.broadcasted_iota(jnp.int32, (tok_rows, tok_rows), 1)
        before = jnp.where(earlier < later, 1.0, 0.0).astype(BF16)
        rank = mm(hit.astype(BF16), before)
        place = jnp.where(hit > 0.0, rank, -1.0)
        place_at[...] = place
        gate_at[...] = gate_of
        place_ref[...] = place

    r = lax.broadcasted_iota(jnp.int32, (cap, tok_rows), 0).astype(F32)
    picks, scales = [], []
    for j in range(block):
        at = pl.ds(step * block + j, 1)
        pick = jnp.broadcast_to(place_at[at, :], (cap, tok_rows)) == r
        picks.append(jnp.where(pick, 1.0, 0.0))
        scales.append(jnp.sum(jnp.where(pick, gate_at[at, :], 0.0), axis=1, keepdims=True))
    select = jnp.concatenate(picks, axis=0).astype(BF16)
    scale = jnp.concatenate(scales, axis=0)
    sent_ref[:, :half] = mm(select, tok_ref[...]).astype(BF16)
    sent_ref[:, half:] = (mm(select, cot_ref[...]) * scale).astype(BF16)


def routing(tp, ids_t, gates_t, tokens, cotangent, experts, cap):
    tok_rows, width = tokens.shape
    half = width // 2
    top = ids_t.shape[0]
    steps = 4
    rows = experts * cap // steps
    return pl.pallas_call(
        routing_kernel,
        grid_spec=pltpu.PrefetchScalarGridSpec(
            num_scalar_prefetch=1,
            grid=(steps,),
            in_specs=[
                pl.BlockSpec((top, tok_rows), lambda i, tp: (0, 0)),
                pl.BlockSpec((top, tok_rows), lambda i, tp: (0, 0)),
                pl.BlockSpec((tok_rows, half), lambda i, tp: (0, tp[0])),
                pl.BlockSpec((tok_rows, half), lambda i, tp: (0, tp[0])),
            ],
            out_specs=[
                pl.BlockSpec((rows, width), lambda i, tp: (i, 0)),
                pl.BlockSpec((experts, tok_rows), lambda i, tp: (0, 0)),
            ],
            scratch_shapes=[pltpu.VMEM((experts, tok_rows), F32), pltpu.VMEM((experts, tok_rows), F32)],
        ),
        out_shape=[
            jax.ShapeDtypeStruct((experts * cap, width), BF16),
            jax.ShapeDtypeStruct((experts, tok_rows), F32),
        ],
        name="routing",
    )(tp.reshape(1), ids_t, gates_t, tokens, cotangent)


def payload_kernel(d_ref, w_ref, peer_ref, out_ref):
    block, lines, lanes = out_ref.shape
    cap = peer_ref.shape[0] // block
    own = mm(d_ref[...], w_ref[...], COLS).astype(BF16).astype(F32)
    both = (own + peer_ref[...].astype(F32)).astype(BF16)
    for e in range(block):
        at = slice(e * cap, (e + 1) * cap)
        for c in range(lines // cap):
            out_ref[e, c * cap : (c + 1) * cap, :] = both[at, c * lanes : (c + 1) * lanes]


def payload_of(d_both, w_own, peer, experts, extra):
    slots, half = peer.shape
    steps = 4
    cap = slots // experts
    lines = cap * half // 128
    return pl.pallas_call(
        payload_kernel,
        grid=(steps,),
        in_specs=[
            pl.BlockSpec((slots // steps, d_both.shape[1]), lambda i: (i, 0)),
            pl.BlockSpec(w_own.shape, lambda i: (0, 0)),
            pl.BlockSpec((slots // steps, half), lambda i: (i, 0)),
        ],
        out_specs=pl.BlockSpec((experts // steps, lines, 128), lambda i: (i, 0, 0)),
        out_shape=jax.ShapeDtypeStruct((experts, lines + extra, 128), BF16),
        compiler_params=pltpu.CompilerParams(vmem_limit_bytes=GRANT),
        name="payload",
    )(d_both, w_own, peer)


def total_kernel(got_ref, notes_ref, payload_ref, down_ref, out_ref):
    down = jnp.sum(got_ref[...].astype(F32), axis=0)
    down_ref[...] = down
    norms = jnp.sum(down * down, axis=0, keepdims=True)
    high = norms.astype(BF16).astype(F32)
    low = norms - high
    lines = out_ref.shape[1:]
    row = lax.broadcasted_iota(jnp.int32, lines, 0)
    marks = jnp.zeros(lines, F32)
    pieces = norms.shape[1] // lines[1]
    for at, value in enumerate((high, low)):
        for c in range(pieces):
            line = value[:, c * lines[1] : (c + 1) * lines[1]]
            marks = jnp.where(row == at * pieces + c, line, marks)
    out_ref[...] = (notes_ref[...] + marks[None]).astype(BF16)


def totals(got, notes, payload):
    size, rows, cols = got.shape
    cols = cols // 3
    experts, extra, lanes = notes.shape
    last = payload.shape[1] // extra - 1
    return pl.pallas_call(
        total_kernel,
        grid=(1,),
        in_specs=[
            pl.BlockSpec((size, rows, cols), lambda i: (0, 0, 2)),
            pl.BlockSpec((experts, extra, lanes), lambda i: (0, 0, 0)),
            pl.BlockSpec(memory_space=pl.ANY),
        ],
        out_specs=[
            pl.BlockSpec((rows, cols), lambda i: (0, 0)),
            pl.BlockSpec((experts, extra, lanes), lambda i: (0, last, 0)),
        ],
        out_shape=[
            jax.ShapeDtypeStruct((rows, cols), F32),
            jax.ShapeDtypeStruct(payload.shape, BF16),
        ],
        input_output_aliases={2: 1},
        compiler_params=pltpu.CompilerParams(vmem_limit_bytes=GRANT),
        name="totals",
    )(got, notes, payload)


def final_kernel(rows_ref, notes_ref, select_ref, own_ref, peer_ref, place_ref, ids_ref, gates_ref, tok_ref, gate_ref, down_ref, gate_at):
    experts, lines, lanes = rows_ref.shape
    tiles = own_ref.shape[1] // lanes
    cap = lines // tiles
    columns = [rows_ref[:, c * cap : (c + 1) * cap, :].reshape(experts * cap, lanes) for c in range(tiles)]
    back = jnp.concatenate(columns, axis=1)
    routed = mm(select_ref[...], back)
    tok_ref[...] = (routed + (own_ref[...].astype(F32) + peer_ref[...].astype(F32))).astype(BF16)

    @pl.when(pl.program_id(0) == 0)
    def _():
        notes = notes_ref[...].astype(F32)
        whole = jnp.sum(notes, axis=0)
        down_ref[...] = jnp.concatenate([whole[0:1] + whole[2:3], whole[1:2] + whole[3:4]], axis=1)
        row = lax.broadcasted_iota(jnp.int32, notes.shape, 1)
        gate_at[...] = jnp.sum(jnp.where((row == 4) | (row == 5), notes, 0.0), axis=1)
        gate = gate_at[...]
        place = place_ref[...]
        at = jnp.zeros(place.shape, F32)
        for r in range(cap):
            at = jnp.where(place == r, gate[:, r : r + 1], at)
        e = lax.broadcasted_iota(jnp.int32, place.shape, 0)
        for k in range(ids_ref.shape[0]):
            mine = jnp.sum(jnp.where(turn_of(ids_ref[k : k + 1, :], experts) == e, at, 0.0), axis=0, keepdims=True)
            gate_ref[k : k + 1, :] = mine / gates_ref[k : k + 1, :]


def finished(payload, select_t, s_own, s_peer, place, ids_t, gates_t):
    experts, lines, lanes = payload.shape
    tok_rows, half = s_own.shape
    slots = select_t.shape[1]
    cap = slots // experts
    steps = 2
    cols = half // steps
    tiles = cols // lanes
    extra = lines - cap * half // lanes
    return pl.pallas_call(
        final_kernel,
        grid=(steps,),
        in_specs=[
            pl.BlockSpec((experts, tiles * cap, lanes), lambda i: (0, i, 0)),
            pl.BlockSpec((experts, extra, lanes), lambda i: (0, lines // extra - 1, 0)),
            pl.BlockSpec((tok_rows, slots), lambda i: (0, 0)),
            pl.BlockSpec((tok_rows, cols), lambda i: (0, i)),
            pl.BlockSpec((tok_rows, cols), lambda i: (0, i)),
            pl.BlockSpec(place.shape, lambda i: (0, 0)),
            pl.BlockSpec(ids_t.shape, lambda i: (0, 0)),
            pl.BlockSpec(gates_t.shape, lambda i: (0, 0)),
        ],
        out_specs=[
            pl.BlockSpec((tok_rows, cols), lambda i: (0, i)),
            pl.BlockSpec(gates_t.shape, lambda i: (0, 0)),
            pl.BlockSpec((1, 2 * lanes), lambda i: (0, 0)),
        ],
        out_shape=[
            jax.ShapeDtypeStruct((tok_rows, half), BF16),
            jax.ShapeDtypeStruct(gates_t.shape, F32),
            jax.ShapeDtypeStruct((1, 2 * lanes), F32),
        ],
        scratch_shapes=[pltpu.VMEM((experts, lanes), F32)],
        compiler_params=pltpu.CompilerParams(vmem_limit_bytes=GRANT),
        name="final",
    )(payload, payload, select_t, s_own, s_peer, place, ids_t, gates_t)


def positions(size):
    return [(i // SIDE**2 % SIDE, i // SIDE % SIDE, i % SIDE) for i in range(size)]


def next_along(x, by):
    pairs = []
    for z, y, x_at in positions(lax.axis_size("ep")):
        here = (z * SIDE + y) * SIDE + x_at
        pairs.append((2 * here, 2 * ((((z + by) % SIDE) * SIDE + y) * SIDE + x_at)))
        pairs.append((2 * here + 1, 2 * ((z * SIDE + (y + by) % SIDE) * SIDE + x_at) + 1))
    return lax.ppermute(x, ("ep", "tp"), pairs)


def plane_groups(size):
    at = positions(size)
    by_z = [[2 * i for i in range(size) if at[i][0] == c] for c in range(SIDE)]
    by_y = [[2 * i + 1 for i in range(size) if at[i][1] == c] for c in range(SIDE)]
    return by_z + by_y


def stage_kernel(a_ref, b_ref, c_ref, d_ref, out_ref):
    pair = a_ref[...].astype(F32) + b_ref[...].astype(F32)
    out_ref[...] = (pair + (c_ref[...].astype(F32) + d_ref[...].astype(F32))).astype(BF16)


def stage_total(pieces):
    rows, cols = pieces[0].shape
    steps = 2
    spec = pl.BlockSpec((rows // steps, cols), lambda i: (i, 0))
    return pl.pallas_call(
        stage_kernel,
        grid=(steps,),
        in_specs=[spec] * len(pieces),
        out_specs=spec,
        out_shape=jax.ShapeDtypeStruct((rows, cols), BF16),
        compiler_params=pltpu.CompilerParams(vmem_limit_bytes=GRANT),
        name="stage_total",
    )(*pieces)


def silu_parts(pre):
    sigmoid = jax.nn.sigmoid(pre)
    return (pre * sigmoid, sigmoid * (1.0 + pre * (1.0 - sigmoid)))


def to_hidden(inputs, cots, w_g, w_u, w_d):
    gate_pre = mm(inputs, w_g)
    up_pre = mm(inputs, w_u)
    active, slope = silu_parts(gate_pre)
    hidden = (active * up_pre).astype(BF16)
    hidden_cot = mm(cots, w_d, COLS)
    gate_part = jnp.sum(hidden.astype(F32) * hidden_cot, axis=1)
    d_gate = (hidden_cot * up_pre * slope).astype(BF16)
    d_up = (hidden_cot * active).astype(BF16)
    return hidden, d_gate, d_up, gate_part


def input_rows(d_both, w_both, first, width):
    return mm(d_both, lax.dynamic_slice_in_dim(w_both, first, width, 0), COLS).astype(BF16)


def layer(tokens, expert_ids, gates, cotangent, w_gate, w_up, w_down, sh_gate, sh_up, sh_down):
    experts = lax.axis_size("ep")
    tok_rows, width = tokens.shape
    top = expert_ids.shape[1]
    cap = 3 * tok_rows * top // (2 * experts)
    slots = experts * cap
    half = width // 2
    tp = lax.axis_index("tp")
    own, other = tp * half, (1 - tp) * half
    w_g, w_u, w_d = w_gate[0], w_up[0], w_down[0]

    ids_t = expert_ids.T
    gates_t = gates.T
    sent, place = routing(tp, ids_t, gates_t, tokens, cotangent, experts, cap)
    got = to_each(sent.reshape(experts, cap, width)).reshape(slots, width)

    s_hidden, s_gate, s_up, _ = to_hidden(tokens, cotangent, sh_gate, sh_up, sh_down)
    hid = s_hidden.shape[1]
    s_both = jnp.concatenate([sh_gate, sh_up], axis=1)
    s_d = jnp.concatenate([s_gate, s_up], axis=1)
    s_other = input_rows(s_d, s_both, other, half)
    s_own = input_rows(s_d, s_both, own, half)
    shared = jnp.concatenate([mm(tokens, s_d, ROWS), mm(cotangent, s_hidden, ROWS)], axis=1).astype(BF16)
    plane = experts // SIDE
    block = width // SIDE**2
    ep = lax.axis_index("ep")
    z, y = lax.div(ep, plane), lax.rem(lax.div(ep, SIDE), SIDE)
    main = jnp.where(tp == 0, z, y)
    step, stride = jnp.where(tp == 0, SIDE, 1), jnp.where(tp == 0, 1, SIDE)
    pieces = []
    for by in range(SIDE):
        first = lax.rem(main + by, SIDE) * step
        pieces.append(
            jnp.concatenate(
                [
                    lax.dynamic_slice_in_dim(shared, (first + j * stride) * block, block, 0)
                    for j in range(SIDE)
                ],
                axis=0,
            )
        )
    arrived = [next_along(pieces[by], by) for by in range(1, SIDE)]
    terms = stage_total(pieces[:1] + arrived).reshape(plane, width // experts, 3 * hid)
    shared_got = lax.all_to_all(
        terms, ("ep", "tp"), 0, 0, tiled=True, axis_index_groups=plane_groups(experts)
    )
    s_peer = swap(s_other)
    w_gu = jnp.concatenate([w_g, w_u], axis=1)
    w_gu_own = lax.dynamic_slice_in_dim(w_gu, own, half, 0)
    w_gu_other = lax.dynamic_slice_in_dim(w_gu, other, half, 0)
    w_d_own = lax.dynamic_slice_in_dim(w_d, own, half, 1)
    w_d_other = lax.dynamic_slice_in_dim(w_d, other, half, 1)

    slot = jnp.arange(slots, dtype=jnp.int32)
    pick = place.T[:, :, None] == (slot[:cap].astype(F32))[None, None, :]
    select_t = pick.astype(BF16).reshape(tok_rows, slots)
    peer = swap(got)
    pre = mm(got[:, :half], w_gu_own) + mm(peer[:, :half], w_gu_other)
    hidden_cot = mm(got[:, half:], w_d_own, COLS) + mm(peer[:, half:], w_d_other, COLS)
    gate_pre, up_pre = pre[:, :hid], pre[:, hid:]
    active, slope = silu_parts(gate_pre)
    hidden = (active * up_pre).astype(BF16)
    gate_part = jnp.sum(hidden.astype(F32) * hidden_cot, axis=1)
    d_both = jnp.concatenate([hidden_cot * up_pre * slope, hidden_cot * active], axis=1).astype(BF16)
    rows_other = mm(d_both, w_gu_other, COLS).astype(BF16)
    from_peer = swap(rows_other)
    gate_peer = swap(gate_part)
    extra = 8
    payload = payload_of(d_both, w_gu_own, from_peer, experts, extra)
    gate_sum = jnp.pad((gate_part + gate_peer).reshape(experts, 1, cap), ((0, 0), (0, 0), (0, 128 - cap)))
    high = lax.reduce_precision(gate_sum, 8, 7)
    line = jnp.arange(extra)[None, :, None]
    notes = jnp.where(line == 4, high, jnp.where(line == 5, gate_sum - high, 0.0))
    down_sum, payload = totals(shared_got, notes, payload)
    back = to_each(payload)
    shared_sum = jnp.sum(shared_got[:, :, : 2 * hid].astype(F32), axis=0)
    shared_g, shared_u = shared_sum[:, :hid], shared_sum[:, hid:]
    shared_d = down_sum.T

    low = tp == 0
    inputs = jnp.concatenate(
        [jnp.where(low, got[:, :half], peer[:, :half]), jnp.where(low, peer[:, :half], got[:, :half])],
        axis=1,
    )
    cots = jnp.concatenate(
        [jnp.where(low, got[:, half:], peer[:, half:]), jnp.where(low, peer[:, half:], got[:, half:])],
        axis=1,
    )
    grad_g = mm(inputs, d_both[:, :hid], ROWS)
    grad_u = mm(inputs, d_both[:, hid:], ROWS)
    grad_d = mm(hidden, cots, ROWS)

    norms = jnp.concatenate(
        [
            jnp.sum(grad_g * grad_g, axis=1),
            jnp.sum(grad_u * grad_u, axis=1),
            jnp.sum(shared_g * shared_g, axis=1),
            jnp.sum(shared_u * shared_u, axis=1),
        ]
    )
    norms = norms + swap(norms)
    step = width // experts
    gate_norms, up_norms = norms[:width], norms[width : 2 * width]
    shared_gate_norms, shared_up_norms = norms[2 * width : 2 * width + step], norms[2 * width + step :]

    token_grad, gate_grad, down_norms = finished(back, select_t, s_own, s_peer, place, ids_t, gates_t)
    gate_grad = gate_grad.T
    down_norms = down_norms.reshape(hid)
    return (
        token_grad,
        gate_grad,
        grad_g[None],
        grad_u[None],
        grad_d[None],
        shared_g,
        shared_u,
        shared_d,
        gate_norms[None],
        up_norms[None],
        jnp.sum(grad_d * grad_d, axis=1)[None],
        shared_gate_norms,
        shared_up_norms,
        down_norms,
    )


def solution(mesh):
    placed = (
        P("ep", None),
        P("ep", None),
        P("ep", None),
        P("ep", None),
        P("ep", None, "tp"),
        P("ep", None, "tp"),
        P("ep", "tp", None),
        P(None, "tp"),
        P(None, "tp"),
        P("tp", None),
    )
    return jax.shard_map(
        layer,
        mesh=mesh,
        in_specs=placed,
        out_specs=(
            P("ep", "tp"),
            P("ep", None),
            P("ep", None, "tp"),
            P("ep", None, "tp"),
            P("ep", "tp", None),
            P("ep", "tp"),
            P("ep", "tp"),
            P("tp", "ep"),
            P("ep", None),
            P("ep", None),
            P("ep", "tp"),
            P("ep"),
            P("ep"),
            P("tp"),
        ),
        check_vma=False,
    )
```
